32 devices in a mesh: sp: 8 (over z, x), tp: 4 (over y, core).
Axes of the slice: x: 2, y: 2, z: 4, core: 2. Of those that a mesh axis runs over, the one named last changes fastest.
Arguments:
- queries: bfloat16 [4096, 512], P('sp', 'tp'), may hold values from -9.5625 to 9.5625
- keys: bfloat16 [4096, 512], P('sp', 'tp'), may hold values from -9.5625 to 9.5625
- values: bfloat16 [4096, 512], P('sp', 'tp'), may hold values from -6 to 6
- key_bias: bfloat16 [4096, 8], P('sp', 'tp'), may hold values from -17 to 0
- residual: bfloat16 [4096, 2048], P(('sp', 'tp')), may hold values from -6 to 6
- out_weight: bfloat16 [512, 2048], replicated, may hold values from -1 to 1
- norm_gain: float32 [2048], replicated, may hold values from 0.1 to 1.9
- routes: int32 [4096, 2], P(('sp', 'tp')), may hold values from 0 to 7, all different within a row; in each aligned block of 128 rows (0 to 127, 128 to 255, ...) at most 40 rows name the same one
- route_weights: float32 [4096, 2], P(('sp', 'tp')), may hold values from 0.25 to 2
- gate_weight: bfloat16 [8, 2048, 4096], P('sp', None, 'tp'), may hold values from -0.125 to 0.125
- up_weight: bfloat16 [8, 2048, 4096], P('sp', None, 'tp'), may hold values from -0.125 to 0.125
- down_weight: bfloat16 [8, 4096, 2048], P('sp', 'tp'), may hold values from -0.09375 to 0.09375
Outputs:
- output: bfloat16 [4096, 2048], P(('sp', 'tp'))
The draws below stay inside these ranges and needn't reach their ends.
Inputs may be any that keep to these rules, and one draw needn't show every extreme that they name: `routes`: each row names 2 different experts; the rows of one device name no expert more than 40 times.
All inputs are finite; a program needn't handle non-finite values.
Results may differ from the reference program's by a relative error of at most 0.017.
Values may be sent and summed in bfloat16 or wider, within the bound.
A program may use at most 128 MiB of HBM per device.

```python
import math
import jax
import jax.numpy as jnp
import numpy as np
from jax import lax

D = 2048
HEAD_COUNT = 8
HEAD_DIM = 64
FF = 4096
TOP = 2
SPAN = 512
TOK_DEV = 128
TOK_SP = 512
SEQUENCE_LENGTH = 4096
EXPERTS = 8
CAP = 40
N_SP = 8
N_TP = 4


def draw_key_bias(key, part):
    gathered_keys = jax.random.split(jax.random.fold_in(key, 7), 6)
    fast_share = 0.5
    is_fast = jax.random.uniform(gathered_keys[0], (HEAD_COUNT,), jnp.float32) < fast_share
    slow_level = -jnp.log(jnp.float32(SEQUENCE_LENGTH)) - 3.0 + jax.random.uniform(gathered_keys[1], (HEAD_COUNT,), jnp.float32, minval=-0.5, maxval=0.5)
    fast_level = jax.random.uniform(gathered_keys[2], (HEAD_COUNT,), jnp.float32, minval=-7.0, maxval=-5.5)
    level = jnp.where(is_fast, fast_level, slow_level)
    block_shift = jnp.repeat(jax.random.uniform(gathered_keys[3], (N_SP,), jnp.float32, minval=-0.7, maxval=0.7), TOK_SP, total_repeat_length=SEQUENCE_LENGTH)
    sudden_position = jax.random.randint(gathered_keys[4], (4,), 0, SEQUENCE_LENGTH)
    sudden_value = jax.random.uniform(gathered_keys[5], (4, HEAD_COUNT), jnp.float32, minval=-1.5, maxval=0.0)
    position_index = jnp.arange(SEQUENCE_LENGTH, dtype=jnp.int32)
    sudden_hit_mask = (position_index[:, None] == sudden_position[None, :]).astype(jnp.float32)
    any_hit_flag = jnp.sum(sudden_hit_mask, axis=1, keepdims=True) > 0.0
    sudden_rows = jnp.dot(sudden_hit_mask, sudden_value)
    regular_rows = level[None, :] + block_shift[:, None]
    return jnp.where(any_hit_flag, sudden_rows, regular_rows).astype(jnp.bfloat16)


def levels(key, extent, pieces, smallest, high):
    factor_of = 1.0
    for position, shards_of in pieces:
        steps = jax.random.uniform(jax.random.fold_in(jax.random.fold_in(key, 6), position), (shards_of,), jnp.float32, smallest / len(pieces), high / len(pieces))
        factor_of = factor_of * jnp.repeat(jnp.exp(steps), extent[position] // shards_of).reshape((-1,) + (1,) * (len(extent) - 1 - position))
    return factor_of


def shared_out(own_key, own, number, rows, number_of, top, most, lean):
    ranking = jax.random.permutation(own_key, number_of)
    crowded, ordinary = load_shares(number_of, rows * top, most, lean, True), load_shares(number_of, rows * top, most, lean, False)
    places = jnp.arange(number_of)

    def named(lengths, offset_by):
        used = int((lengths > 0).sum())
        fixed = max(1, used // 4)
        shifted = fixed + (places - fixed + offset_by * (used - fixed)) % max(1, number_of - fixed)
        return jnp.zeros((number_of,), jnp.int32).at[ranking[jnp.where(places < fixed, places, shifted)]].set(jnp.asarray(lengths, jnp.int32))

    lengths = jnp.where(number % 4 == 0, named(crowded, number // 4), named(ordinary, number - number // 4 - 1))
    mixed = jax.random.permutation(jax.random.fold_in(own, 3), number_of)
    source_of, taker = mixed[0:number_of // 2 * 2:2], mixed[1:number_of // 2 * 2:2]
    room = jnp.minimum(lengths[source_of] - 1, most - lengths[taker]) // 2
    room = jnp.where((source_of == ranking[0]) | (taker == ranking[0]) | (lengths[taker] == 0), 0, jnp.maximum(room, 0))
    shifted = jax.random.randint(jax.random.fold_in(own, 4), (number_of // 2,), 0, 1 << 20) % (room + 1)
    lengths = lengths.at[source_of].add(-shifted).at[taker].add(shifted)
    labels = jnp.searchsorted(jnp.cumsum(lengths), jnp.arange(rows * top), side="right").astype(jnp.int32)
    table = labels.reshape(top, rows).T
    table = table[jax.random.permutation(jax.random.fold_in(own, 1), rows)]
    offset_by = jax.random.randint(jax.random.fold_in(own, 2), (rows, 1), 0, top)
    return jnp.take_along_axis(table, (jnp.arange(top)[None, :] + offset_by) % top, axis=1)


def load_shares(amount, total, reach, slope, full):
    portions = [(1 << 20) // math.isqrt(rank ** slope) + 1 for rank in range(1, amount + 1)]
    largest = reach if full else min(reach, max(-(-total // amount), total * portions[0] // sum(portions)))
    least = 1 if total - largest >= amount - 1 else 0
    given, rest = [largest] + [least] * (amount - 1), total - largest - least * (amount - 1)
    while rest > 0:
        candidates = [i for i in range(1, amount) if given[i] < largest] or [i for i in range(1, amount) if given[i] < reach]
        whole, left = sum([portions[i] for i in candidates]), rest
        for i in candidates:
            more = min(reach - given[i], max(1, left * portions[i] // whole), rest)
            given[i] = given[i] + more
            rest = rest - more
    return np.array(given)


def normal_values(rng, shape, width, bound, pieces=(), held_as=jnp.bfloat16):
    result = jax.random.normal(rng, shape, jnp.float32) * width
    if len(pieces) > 0:
        result = levels(rng, shape, pieces, -0.22, 0.18) * result
    return jnp.clip(result, min=-bound, max=bound).astype(held_as)


def setup_inputs(seed: int = 0) -> dict:
    splits = jax.random.split(jax.random.key(seed), 13)
    queries = normal_values(splits[0], (SEQUENCE_LENGTH, HEAD_COUNT * HEAD_DIM), 1.6, 9.5625, ((0, 8), (1, 4)))
    keys = normal_values(splits[1], (SEQUENCE_LENGTH, HEAD_COUNT * HEAD_DIM), 1.6, 9.5625, ((0, 8), (1, 4)))
    values = normal_values(splits[2], (SEQUENCE_LENGTH, HEAD_COUNT * HEAD_DIM), 1.0, 6.0, ((0, 8), (1, 4)))
    key_bias = draw_key_bias(jax.random.fold_in(splits[12], 71), 0)
    residual = normal_values(splits[4], (SEQUENCE_LENGTH, D), 1.0, 6.0, ((0, 32),))
    out_weight = normal_values(splits[5], (HEAD_COUNT * HEAD_DIM, D), (HEAD_COUNT * HEAD_DIM // 16) ** -0.5, 1.0)
    norm_gain = jnp.clip(1.0 + 0.18 * jax.random.normal(splits[6], (D,), jnp.float32), 0.1, 1.9)
    routes_keys = jax.random.split(jax.random.fold_in(splits[7], 1), SEQUENCE_LENGTH // TOK_DEV)
    routes_turns = jax.random.permutation(jax.random.fold_in(splits[7], 3), SEQUENCE_LENGTH // TOK_DEV)
    routes = jax.vmap(lambda own, number: shared_out(jax.random.fold_in(splits[7], 2), own, number, TOK_DEV, EXPERTS, TOP, CAP, 1))(routes_keys, routes_turns).reshape((SEQUENCE_LENGTH, TOP))
    route_weights = jnp.clip(jnp.exp(math.log(2.0) - 2.0794415 * jax.random.uniform(splits[8], (SEQUENCE_LENGTH, TOP), jnp.float32) ** levels(splits[8], (SEQUENCE_LENGTH, TOP), ((0, 32),), -0.2, 0.2)), 0.25, 2.0)
    gate_weight = normal_values(splits[9], (EXPERTS, D, FF), D ** -0.5, 0.125, ((0, 8), (2, 4)))
    up_weight = normal_values(splits[10], (EXPERTS, D, FF), D ** -0.5, 0.125, ((0, 8), (2, 4)))
    down_weight = normal_values(splits[11], (EXPERTS, FF, D), FF ** -0.5, 0.09375, ((0, 8), (1, 4)))
    return {"queries": queries, "keys": keys, "values": values, "key_bias": key_bias, "residual": residual, "out_weight": out_weight, "norm_gain": norm_gain, "routes": routes, "route_weights": route_weights, "gate_weight": gate_weight, "up_weight": up_weight, "down_weight": down_weight}


epsilon = 1e-06

def stick_span(query_block, key_block, value_block, bias_block, query_pos, key_pos):
    scores = jnp.einsum('qhd,khd->qhk', query_block, key_block) * HEAD_DIM ** (-0.5)
    scores = scores + jnp.transpose(bias_block)[None, :, :]
    earlier = key_pos[None, None, :] < query_pos[:, None, None]
    failure = jnp.where(earlier, jax.nn.log_sigmoid(-scores), 0.0)
    later_sum = lax.cumsum(failure, axis=2, reverse=True) - failure
    weights = jnp.where(earlier, jnp.exp(jax.nn.log_sigmoid(scores) + later_sum), 0.0).astype(jnp.bfloat16)
    span_out = jnp.einsum('qhk,khd->qhd', weights.astype(jnp.float32), value_block)
    return (span_out, lax.optimization_barrier(jnp.sum(failure, axis=2)))

def attend(queries, keys, values, key_bias):
    span_count = SEQUENCE_LENGTH // SPAN
    query_spans = queries.astype(jnp.float32).reshape(span_count, SPAN, HEAD_COUNT, HEAD_DIM)
    key_spans = keys.astype(jnp.float32).reshape(span_count, SPAN, HEAD_COUNT, HEAD_DIM)
    value_spans = values.astype(jnp.float32).reshape(span_count, SPAN, HEAD_COUNT, HEAD_DIM)
    bias_spans = key_bias.astype(jnp.float32).reshape(span_count, SPAN, HEAD_COUNT)

    def per_block(inputs):
        query_block, block_index = inputs
        query_pos = block_index * SPAN + jnp.arange(SPAN, dtype=jnp.int32)

        def step(held, key_index):
            running, after_total = held

            def compute():
                key_pos = key_index * SPAN + jnp.arange(SPAN, dtype=jnp.int32)
                return stick_span(query_block, key_spans[key_index], value_spans[key_index], bias_spans[key_index], query_pos, key_pos)

            def skipped():
                return (jnp.zeros((SPAN, HEAD_COUNT, HEAD_DIM), jnp.float32), jnp.zeros((SPAN, HEAD_COUNT), jnp.float32))
            span_out, span_sum = lax.cond(key_index <= block_index, compute, skipped)
            return ((running + jnp.exp(after_total)[..., None] * span_out, after_total + span_sum), None)
        start_pair = (jnp.zeros((SPAN, HEAD_COUNT, HEAD_DIM), jnp.float32), jnp.zeros((SPAN, HEAD_COUNT), jnp.float32))
        (running, _), _ = lax.scan(step, start_pair, jnp.arange(span_count, dtype=jnp.int32), reverse=True)
        return running.astype(jnp.bfloat16)
    blocks = lax.map(per_block, (query_spans, jnp.arange(span_count, dtype=jnp.int32)))
    return blocks.reshape(SEQUENCE_LENGTH, HEAD_COUNT * HEAD_DIM)

def experts_out(normed, routes, route_weights, gate_weight, up_weight, down_weight):
    most_rows = SEQUENCE_LENGTH // TOK_DEV * CAP
    flat_routes = routes.reshape(-1)
    flat_weights = route_weights.reshape(-1)
    token_of = (jnp.arange(SEQUENCE_LENGTH * TOP, dtype=jnp.int32) // TOP).astype(jnp.int32)
    block_units = FF // N_TP

    def one_expert(total, expert_index):
        chosen = flat_routes == expert_index
        picked = jnp.nonzero(chosen, size=most_rows, fill_value=0)[0].astype(jnp.int32)
        row_valid = jnp.arange(most_rows, dtype=jnp.int32) < jnp.sum(chosen.astype(jnp.int32))
        token_ids = token_of[picked]
        row_block = normed[token_ids]
        gate_act = jnp.dot(row_block, gate_weight[expert_index], preferred_element_type=jnp.float32)
        up_act = jnp.dot(row_block, up_weight[expert_index], preferred_element_type=jnp.float32)
        hidden = (jax.nn.silu(gate_act) * up_act).astype(jnp.bfloat16)
        summed = jnp.zeros((most_rows, D), jnp.float32)
        for block in range(N_TP):
            lower = block * block_units
            partial_value = jnp.dot(hidden[:, lower:lower + block_units], down_weight[expert_index, lower:lower + block_units], preferred_element_type=jnp.float32)
            summed = summed + lax.optimization_barrier(partial_value.astype(jnp.bfloat16)).astype(jnp.float32)
        expert_rows = lax.optimization_barrier(summed.astype(jnp.bfloat16)).astype(jnp.float32)
        scaled = jnp.where(row_valid[:, None], flat_weights[picked][:, None] * expert_rows, 0.0)
        return (total.at[token_ids].add(scaled), None)
    routed, _ = lax.scan(one_expert, jnp.zeros((SEQUENCE_LENGTH, D), jnp.float32), jnp.arange(EXPERTS, dtype=jnp.int32))
    return routed

def reference(queries, keys, values, key_bias, residual, out_weight, norm_gain, routes, route_weights, gate_weight, up_weight, down_weight):
    attended = attend(queries, keys, values, key_bias)
    mixed_rows = (residual.astype(jnp.float32) + jnp.dot(attended, out_weight, preferred_element_type=jnp.float32)).astype(jnp.bfloat16)
    stream = mixed_rows.astype(jnp.float32)
    normed = (stream * lax.rsqrt(lax.optimization_barrier(jnp.mean(stream * stream, axis=-1, keepdims=True)) + epsilon) * norm_gain).astype(jnp.bfloat16)
    routed = experts_out(normed, routes, route_weights, gate_weight, up_weight, down_weight)
    return (stream + routed).astype(jnp.bfloat16)
```

```python
import functools

import jax
import jax.numpy as jnp
from jax import lax
from jax.experimental import pallas as pl
from jax.experimental.pallas import tpu as pltpu
from jax.sharding import PartitionSpec as P

HEAD_DIM = 64
TOP = 2
SPAN = 512
BLOCK = 256
QUERY_ROWS = 256
BIAS_ROWS = 16
PAIR = 2 * HEAD_DIM
MESH = pl.DeviceIdType.MESH


epsilon = 1e-06


def attend_kernel(
    n, length, heads, q_ref, own_ref, out_ref, held, total, after, tri, up_sem, side_sem, recv_sem
):
    me = lax.axis_index("sp")
    odd = lax.rem(me, 2)
    level = me // 2
    partner = me + 1 - 2 * odd
    has_up = me + 2 < n
    has_down = me >= 2
    barrier = pltpu.get_barrier_semaphore()

    def greet(device):
        pl.semaphore_signal(barrier, inc=1, device_id={"sp": device}, device_id_type=MESH)

    greet(partner)
    pl.when(has_up)(lambda: greet(me + 2))
    pl.when(has_down)(lambda: greet(me - 2))

    total[...] = jnp.zeros_like(total)
    after[...] = jnp.zeros_like(after)
    tri_row = lax.broadcasted_iota(jnp.int32, (BLOCK, BLOCK), 0)
    tri_col = lax.broadcasted_iota(jnp.int32, (BLOCK, BLOCK), 1)
    tri[...] = (tri_row > tri_col).astype(jnp.float32).astype(jnp.bfloat16)

    pl.semaphore_wait(barrier, 1 + has_up.astype(jnp.int32) + has_down.astype(jnp.int32))

    def up(d, h, source):
        return pltpu.make_async_remote_copy(
            src_ref=source,
            dst_ref=held.at[(d + 2) * heads + h],
            send_sem=up_sem.at[d * heads + h],
            recv_sem=recv_sem.at[(d + 2) * heads + h],
            device_id={"sp": me + 2},
            device_id_type=MESH,
        )

    def side(d, h, slot, source):
        return pltpu.make_async_remote_copy(
            src_ref=source,
            dst_ref=held.at[slot * heads + h],
            send_sem=side_sem.at[d * heads + h],
            recv_sem=recv_sem.at[slot * heads + h],
            device_id={"sp": partner},
            device_id_type=MESH,
        )

    def send(d, h, source):
        pl.when(has_up)(lambda: up(d, h, source).start())
        pl.when(odd == 0)(lambda: side(d, h, d + 1, source).start())
        pl.when((odd == 1) & (d >= 2))(lambda: side(d, h, d - 1, source).start())

    def sent(d, h, source):
        pl.when(has_up)(lambda: up(d, h, source).wait_send())
        pl.when(odd == 0)(lambda: side(d, h, d + 1, source).wait_send())
        pl.when((odd == 1) & (d >= 2))(lambda: side(d, h, d - 1, source).wait_send())

    def arrived(d, h):
        pltpu.make_async_remote_copy(
            src_ref=held.at[d * heads + h],
            dst_ref=held.at[d * heads + h],
            send_sem=up_sem.at[d * heads + h],
            recv_sem=recv_sem.at[d * heads + h],
            device_id={"sp": partner},
            device_id_type=MESH,
        ).wait_recv()

    per_block = BLOCK // PAIR

    def attend_rows(sources, q0, todo, masked):
        rows = pl.ds(q0, QUERY_ROWS)
        units = [(h, block) for block in todo for h in range(heads)]
        rest, soft, beyond = {}, {}, {}
        earlier = None
        if masked is not None:
            earlier = lax.broadcasted_iota(
                jnp.int32, (QUERY_ROWS, BLOCK), 1
            ) < lax.broadcasted_iota(jnp.int32, (QUERY_ROWS, BLOCK), 0)
        for h, block in units:
            b0 = block * BLOCK
            bias = sources[h][length : length + BIAS_ROWS, :].astype(jnp.float32)
            bias_row = jnp.concatenate(
                [
                    bias[block * per_block + i : block * per_block + i + 1]
                    for i in range(per_block)
                ],
                axis=1,
            )
            scores = lax.dot_general(
                q_ref[h, rows, :],
                sources[h][b0 : b0 + BLOCK, :],
                (((1,), (1,)), ((), ())),
                preferred_element_type=jnp.float32,
            )
            scores = scores + bias_row
            value = jnp.maximum(scores, 0.0) + jnp.log(1.0 + jnp.exp(-jnp.abs(scores)))
            rest[h, block] = scores - value
            if block == masked:
                value = jnp.where(earlier, value, 0.0)
            soft[h, block] = value
            beyond[h, block] = jnp.dot(
                value.astype(jnp.bfloat16), tri[...], preferred_element_type=jnp.float32
            )
        for h in range(heads):
            later = after[h, rows, :]
            gathered = total[h, rows, :]
            for block in todo:
                b0 = block * BLOCK
                past = beyond[h, block]
                piece = jnp.exp(rest[h, block] - past - jnp.concatenate([later] * per_block, axis=1))
                if block == masked:
                    piece = jnp.where(earlier, piece, 0.0)
                gathered = gathered + jnp.dot(
                    piece.astype(jnp.bfloat16),
                    sources[h][b0 : b0 + BLOCK, :],
                    preferred_element_type=jnp.float32,
                )
                later = later + (past[:, :1] + soft[h, block][:, :1])
            total[h, rows, :] = gathered
            after[h, rows, :] = later

    blocks = length // BLOCK

    def compute_own():
        sources = [own_ref.at[h] for h in range(heads)]
        for c in range(blocks):
            attend_rows(sources, c * BLOCK, list(reversed(range(c + 1))), c)

    def compute(d):
        sources = [held.at[d * heads + h] for h in range(heads)]

        def chunk(c, carry):
            q0 = pl.multiple_of(c * QUERY_ROWS, QUERY_ROWS)
            attend_rows(sources, q0, list(reversed(range(blocks))), None)
            return carry

        lax.fori_loop(0, length // QUERY_ROWS, chunk, 0)

    for h in range(heads):
        send(0, h, own_ref.at[h])
    compute_own()

    def step(k, carry):
        @pl.when(k <= level)
        def _():
            for h in range(heads):
                arrived(2 * k, h)
                send(2 * k, h, held.at[2 * k * heads + h])

        first = 2 * k - 3 + 2 * odd

        @pl.when(first >= 1)
        def _():
            for h in range(heads):
                arrived(first, h)

        def one(d, inner):
            compute(d)
            return inner

        lax.fori_loop(jnp.maximum(first, 1), jnp.minimum(first + 1, me) + 1, one, 0)
        return carry

    lax.fori_loop(1, level + 2, step, 0)
    lane = lax.broadcasted_iota(jnp.int32, (length, PAIR), 1)
    for h in range(0, heads, 2):
        joined = total[h]
        if h + 1 < heads:
            joined = jnp.where(lane >= HEAD_DIM, total[h + 1], joined)
        columns = min(PAIR, (heads - h) * HEAD_DIM)
        out_ref[:, h * HEAD_DIM : h * HEAD_DIM + columns] = joined[:, :columns].astype(jnp.bfloat16)

    for h in range(heads):
        sent(0, h, own_ref.at[h])

    def drain(k, carry):
        for h in range(heads):
            sent(2 * k, h, held.at[2 * k * heads + h])
        return carry

    lax.fori_loop(1, level + 1, drain, 0)


def attend(queries, keys, values, key_bias):
    n = lax.axis_size("sp")
    length = queries.shape[0]
    heads = key_bias.shape[1]
    width = heads * HEAD_DIM
    scaled = queries * jnp.bfloat16(HEAD_DIM ** (-0.5))
    bias_rows = jnp.transpose(key_bias).reshape(heads, -1, PAIR)
    bias_rows = jnp.pad(bias_rows, ((0, 0), (0, BIAS_ROWS - bias_rows.shape[1]), (0, 0)))
    nothing = jnp.zeros((length, HEAD_DIM), queries.dtype)
    per_head, own = [], []
    for h in range(heads):
        columns = slice(h * HEAD_DIM, (h + 1) * HEAD_DIM)
        order = 1 if h % 2 == 0 else -1
        per_head.append(jnp.concatenate([nothing, scaled[:, columns]][::order], axis=1))
        own.append(jnp.concatenate([values[:, columns], keys[:, columns]][::order], axis=1))
    own = jnp.concatenate([jnp.stack(own), bias_rows], axis=1)
    vmem = pl.BlockSpec(memory_space=pltpu.VMEM)
    return pl.pallas_call(
        functools.partial(attend_kernel, n, length, heads),
        out_shape=jax.ShapeDtypeStruct((length, width), jnp.bfloat16),
        in_specs=[vmem, vmem],
        out_specs=vmem,
        scratch_shapes=[
            pltpu.VMEM(((n + 1) * heads, length + BIAS_ROWS, PAIR), jnp.bfloat16),
            pltpu.VMEM((heads, length, PAIR), jnp.float32),
            pltpu.VMEM((heads, length, PAIR), jnp.float32),
            pltpu.VMEM((BLOCK, BLOCK), jnp.bfloat16),
            pltpu.SemaphoreType.DMA(((n + 2) * heads,)),
            pltpu.SemaphoreType.DMA(((n + 2) * heads,)),
            pltpu.SemaphoreType.DMA(((n + 2) * heads,)),
        ],
        compiler_params=pltpu.CompilerParams(
            collective_id=0, has_side_effects=True, vmem_limit_bytes=40 * 1024 * 1024
        ),
        name="attend",
    )(jnp.stack(per_head), own)


def dispatch_kernel(
    n, groups, outgoing, gate_hbm, up_hbm, down_hbm, back, partial, rows, block, hidden, gate, up,
    down, pair, other, done, weight_sem, sp_sem, chip_sem, core_sem, recv_sem, pair_send, pair_recv,
    chip_send, chip_recv, back_send, back_recv,
):
    me, my_t = lax.axis_index("sp"), lax.axis_index("tp")
    core = lax.rem(my_t, 2)
    mate = my_t + 1 - 2 * core
    chips = groups // 2
    alike = [lax.rem(my_t + 2 * k, groups) for k in range(1, chips)]
    loads = [
        pltpu.make_async_copy(gate_hbm, gate, weight_sem.at[0]),
        pltpu.make_async_copy(up_hbm, up, weight_sem.at[1]),
        pltpu.make_async_copy(down_hbm, down, weight_sem.at[2]),
    ]
    for load in loads:
        load.start()
    greet_all(n, me, mate, alike)
    capacity = outgoing.shape[1]

    def copy(source, t, s, send_sem, device):
        return pltpu.make_async_remote_copy(
            src_ref=source,
            dst_ref=rows.at[t * n + s],
            send_sem=send_sem,
            recv_sem=recv_sem.at[t * n + s],
            device_id=device,
            device_id_type=MESH,
        )

    def to_expert(r):
        target = lax.rem(me + r, n)
        return copy(outgoing.at[target], my_t, me, sp_sem.at[r], {"sp": target})

    def to_chip(k, s, source):
        return copy(source, my_t, s, chip_sem.at[k * n + s], {"tp": alike[k]})

    def to_mate(t, s, source):
        return copy(source, t, s, core_sem.at[t * n + s], {"tp": mate})

    def arrived(t, s):
        copy(rows.at[t * n + s], t, s, core_sem.at[t * n + s], {"tp": mate}).wait_recv()

    def spread(s, source):
        for k in range(chips - 1):
            to_chip(k, s, source).start()
        to_mate(my_t, s, source).start()

    def relay(r):
        s = lax.rem(me + n - r, n)
        for t in alike:
            arrived(t, s)
            to_mate(t, s, rows.at[t * n + s]).start()

    def issue(r, carry):
        to_expert(r).start()
        return carry

    spread(me, outgoing.at[me])
    lax.fori_loop(1, n, issue, 0)
    rows[my_t * n + me] = outgoing[me]

    def expert(r):
        s = lax.rem(me + n - r, n)
        arrived(mate, s)
        for t in alike:
            arrived(t + 1 - 2 * lax.rem(t, 2), s)
        block[...] = jnp.concatenate([rows[t * n + s] for t in range(groups)], axis=0)

        def units(f, carry):
            columns = pl.ds(pl.multiple_of(f * BLOCK, BLOCK), BLOCK)
            gate_act = jnp.dot(block[...], gate[:, columns], preferred_element_type=jnp.float32)
            up_act = jnp.dot(block[...], up[:, columns], preferred_element_type=jnp.float32)
            silu = gate_act / (1.0 + jnp.exp(-gate_act))
            hidden[:, columns] = (silu * up_act).astype(jnp.bfloat16)
            return carry

        lax.fori_loop(0, gate.shape[1] // BLOCK, units, 0)

        def features(f, carry):
            columns = pl.ds(pl.multiple_of(f * BLOCK, BLOCK), BLOCK)
            value = jnp.dot(hidden[...], down[:, columns], preferred_element_type=jnp.float32)
            for t in range(groups):
                piece = value[t * capacity : (t + 1) * capacity]
                partial[t * n + s, :, columns] = piece.astype(jnp.bfloat16)
            return carry

        lax.fori_loop(0, down.shape[1] // BLOCK, features, 0)

    def home(r):
        return lax.rem(me + n - r, n)

    def pair_copy(chip, r):
        return pltpu.make_async_remote_copy(
            src_ref=partial.at[(2 * chip + 1 - core) * n + home(r)],
            dst_ref=pair.at[chip * n + r],
            send_sem=pair_send.at[chip * n + r],
            recv_sem=pair_recv.at[chip * n + r],
            device_id={"tp": mate},
            device_id_type=MESH,
        )

    def chip_copy(k, r):
        return pltpu.make_async_remote_copy(
            src_ref=pair.at[(alike[k] // 2) * n + r],
            dst_ref=other.at[k * n + r],
            send_sem=chip_send.at[k * n + r],
            recv_sem=chip_recv.at[k * n + r],
            device_id={"tp": alike[k]},
            device_id_type=MESH,
        )

    def back_copy(r):
        return pltpu.make_async_remote_copy(
            src_ref=done.at[r],
            dst_ref=back.at[me],
            send_sem=back_send.at[r],
            recv_sem=back_recv.at[me],
            device_id={"sp": home(r)},
            device_id_type=MESH,
        )

    def add_pairs(r):
        for chip in range(chips):
            pair_copy(chip, r).wait_recv()
        for k in range(chips - 1):
            chip = alike[k] // 2
            pair[chip * n + r] = (
                partial[alike[k] * n + home(r)].astype(jnp.float32)
                + pair[chip * n + r].astype(jnp.float32)
            ).astype(jnp.bfloat16)

    def add_chips(r):
        value = partial[my_t * n + home(r)].astype(jnp.float32) + pair[
            (my_t // 2) * n + r
        ].astype(jnp.float32)
        for k in range(chips - 1):
            chip_copy(k, r).wait_recv()
            value = value + other[k * n + r].astype(jnp.float32)
        return value.astype(jnp.bfloat16)

    def send_chips(r):
        for k in range(chips - 1):
            chip_copy(k, r).start()

    def multiply(r):
        expert(r)
        for chip in range(chips):
            pair_copy(chip, r).start()

    def sum_pairs(r):
        add_pairs(r)
        send_chips(r)

    def give_own():
        back[me] = add_chips(0)

    def give_back(r):
        done[r] = add_chips(r)
        back_copy(r).start()

    def flow(r):
        pl.when(r < n)(lambda: multiply(r))
        pl.when((r >= 1) & (r <= n))(lambda: sum_pairs(r - 1))
        pl.when(r == 2)(give_own)
        pl.when(r >= 3)(lambda: give_back(r - 2))

    def step(r, carry):
        s = lax.rem(me + n - r, n)
        arrived(my_t, s)
        spread(s, rows.at[my_t * n + s])
        relay(r - 1)
        pl.when(r >= 2)(lambda: flow(r - 2))
        return carry

    lax.fori_loop(1, 2, step, 0)
    for load in loads:
        load.wait()
    lax.fori_loop(2, n, step, 0)
    relay(n - 1)

    def last(r, carry):
        flow(r)
        return carry

    lax.fori_loop(n - 2, n + 2, last, 0)

    def finish(s, carry):
        pl.when(s >= 1)(lambda: to_expert(s).wait_send())
        for k in range(chips - 1):
            to_chip(k, s, outgoing.at[me]).wait_send()
            to_mate(alike[k], s, outgoing.at[me]).wait_send()
        to_mate(my_t, s, outgoing.at[me]).wait_send()
        return carry

    lax.fori_loop(0, n, finish, 0)

    def finish_sums(r, carry):
        for chip in range(chips):
            pair_copy(chip, r).wait_send()
        for k in range(chips - 1):
            chip_copy(k, r).wait_send()
        return carry

    lax.fori_loop(0, n, finish_sums, 0)

    def finish_back(r, carry):
        back_copy(r).wait_send()
        source = home(r)
        pltpu.make_async_remote_copy(
            src_ref=done.at[r],
            dst_ref=back.at[source],
            send_sem=back_send.at[r],
            recv_sem=back_recv.at[source],
            device_id={"sp": source},
            device_id_type=MESH,
        ).wait_recv()
        return carry

    lax.fori_loop(1, n, finish_back, 0)


def greet_all(n, me, mate, alike):
    barrier = pltpu.get_barrier_semaphore()

    def greet(device):
        pl.semaphore_signal(barrier, inc=1, device_id=device, device_id_type=MESH)

    def greet_sp(r, carry):
        greet({"sp": lax.rem(me + r, n)})
        return carry

    lax.fori_loop(1, n, greet_sp, 0)
    greet({"tp": mate})
    for t in alike:
        greet({"tp": t})
    pl.semaphore_wait(barrier, n + len(alike))


def dispatch(outgoing, gate, up, down):
    n, groups = lax.axis_size("sp"), lax.axis_size("tp")
    chips = groups // 2
    _, capacity, width = outgoing.shape
    units = gate.shape[1]
    apart = max(1, chips - 1) * n
    vmem = pl.BlockSpec(memory_space=pltpu.VMEM)
    anywhere = pl.BlockSpec(memory_space=pl.ANY)
    return pl.pallas_call(
        functools.partial(dispatch_kernel, n, groups),
        out_shape=jax.ShapeDtypeStruct((n, capacity, width), outgoing.dtype),
        in_specs=[vmem, anywhere, anywhere, anywhere],
        out_specs=vmem,
        scratch_shapes=[
            pltpu.VMEM((groups * n, capacity, width), outgoing.dtype),
            pltpu.VMEM((groups * n, capacity, width), outgoing.dtype),
            pltpu.VMEM((groups * capacity, width), outgoing.dtype),
            pltpu.VMEM((groups * capacity, units), outgoing.dtype),
            pltpu.VMEM((width, units), gate.dtype),
            pltpu.VMEM((width, units), up.dtype),
            pltpu.VMEM((units, width), down.dtype),
            pltpu.VMEM((chips * n, capacity, width), outgoing.dtype),
            pltpu.VMEM((apart, capacity, width), outgoing.dtype),
            pltpu.VMEM((n, capacity, width), outgoing.dtype),
            pltpu.SemaphoreType.DMA((3,)),
            pltpu.SemaphoreType.DMA((n,)),
            pltpu.SemaphoreType.DMA((max(1, chips - 1) * n,)),
            pltpu.SemaphoreType.DMA((groups * n,)),
            pltpu.SemaphoreType.DMA((groups * n,)),
            pltpu.SemaphoreType.DMA((chips * n,)),
            pltpu.SemaphoreType.DMA((chips * n,)),
            pltpu.SemaphoreType.DMA((apart,)),
            pltpu.SemaphoreType.DMA((apart,)),
            pltpu.SemaphoreType.DMA((n,)),
            pltpu.SemaphoreType.DMA((n,)),
        ],
        compiler_params=pltpu.CompilerParams(
            collective_id=1, has_side_effects=True, vmem_limit_bytes=60 * 1024 * 1024
        ),
        name="dispatch",
    )(outgoing, gate, up, down)


def shards(
    queries,
    keys,
    values,
    key_bias,
    residual,
    out_weight,
    norm_gain,
    routes,
    route_weights,
    gate_weight,
    up_weight,
    down_weight,
):
    sp_count = lax.axis_size("sp")
    attended = attend(queries, keys, values, key_bias)
    token_heads = lax.all_to_all(attended, "tp", split_axis=0, concat_axis=1, tiled=True)
    projected = jnp.dot(token_heads, out_weight, preferred_element_type=jnp.float32)
    stream = (residual.astype(jnp.float32) + projected).astype(jnp.bfloat16).astype(jnp.float32)
    normed = (
        stream * lax.rsqrt(jnp.mean(stream * stream, axis=-1, keepdims=True) + epsilon) * norm_gain
    ).astype(jnp.bfloat16)
    token_count = residual.shape[0]
    width_model = residual.shape[1]
    capacity = max(2, 5 * token_count * TOP // (4 * sp_count))
    flat_routes = routes.reshape(-1)
    onehot = (flat_routes[:, None] == lax.iota(jnp.int32, sp_count)[None, :]).astype(jnp.int32)
    before = jnp.cumsum(onehot, axis=0) - onehot
    slot_of = flat_routes * capacity + jnp.sum(before * onehot, axis=1)
    select = (slot_of[:, None] == lax.iota(jnp.int32, sp_count * capacity)[None, :]).astype(
        jnp.bfloat16
    )
    placing = jnp.sum(select.reshape(token_count, TOP, sp_count * capacity), axis=1)
    outgoing = jnp.einsum("ts,td->sd", placing, normed, preferred_element_type=jnp.float32).astype(
        jnp.bfloat16
    )
    returned = dispatch(
        outgoing.reshape(sp_count, capacity, width_model),
        gate_weight[0],
        up_weight[0],
        down_weight[0],
    ).reshape(-1, width_model)
    picked = jnp.dot(select, returned, preferred_element_type=jnp.float32).reshape(
        token_count, TOP, width_model
    )
    routed = jnp.sum(picked * route_weights[:, :, None], axis=1)
    return (stream + routed).astype(jnp.bfloat16)


def solution(mesh):
    return jax.shard_map(
        shards,
        mesh=mesh,
        in_specs=(
            P("sp", "tp"),
            P("sp", "tp"),
            P("sp", "tp"),
            P("sp", "tp"),
            P(("sp", "tp"), None),
            P(),
            P(),
            P(("sp", "tp"), None),
            P(("sp", "tp"), None),
            P("sp", None, "tp"),
            P("sp", None, "tp"),
            P("sp", "tp", None),
        ),
        out_specs=P(("sp", "tp"), None),
        check_vma=False,
    )
```

```python
import functools

import jax
import jax.numpy as jnp
from jax import lax
from jax.experimental import pallas as pl
from jax.experimental.pallas import tpu as pltpu
from jax.sharding import PartitionSpec as P

HEAD_DIM = 64
TOP = 2
SPAN = 512
BLOCK = 256
QUERY_ROWS = 256
BIAS_ROWS = 16
PAIR = 2 * HEAD_DIM
WIDE = 512
UNITS = 512
FEATURES = 1024
MESH = pl.DeviceIdType.MESH


epsilon = 1e-06


def layer_kernel(
    n, groups, length, heads,
    q_ref, own_ref, place, residual, out_weight, gain, gate_hbm, up_hbm, down_hbm,
    back, mixed,
    held, total, after, tri, attended, heads_in, outgoing, rows, partial, block, hidden,
    gate, up_w, down, pair, other, done,
    up_sem, side_sem, recv_sem, share_send, share_recv, weight_sem, sp_sem, chip_sem, core_sem,
    row_sem, pair_send, pair_recv, chip_send, chip_recv, back_send, back_recv,
):
    me, my_t = lax.axis_index("sp"), lax.axis_index("tp")
    odd = lax.rem(me, 2)
    level = me // 2
    partner = me + 1 - 2 * odd
    has_up = me + 2 < n
    core = lax.rem(my_t, 2)
    mate = my_t + 1 - 2 * core
    chips = groups // 2
    alike = [lax.rem(my_t + 2 * k, groups) for k in range(1, chips)]
    loads = [
        pltpu.make_async_copy(gate_hbm, gate, weight_sem.at[0]),
        pltpu.make_async_copy(up_hbm, up_w, weight_sem.at[1]),
        pltpu.make_async_copy(down_hbm, down, weight_sem.at[2]),
    ]
    greet_all(n, groups, me, my_t)
    total[...] = jnp.zeros_like(total)
    after[...] = jnp.zeros_like(after)
    tri_row = lax.broadcasted_iota(jnp.int32, (BLOCK, BLOCK), 0)
    tri_col = lax.broadcasted_iota(jnp.int32, (BLOCK, BLOCK), 1)
    tri[...] = (tri_row > tri_col).astype(jnp.float32).astype(jnp.bfloat16)

    def up(d, h, source):
        return pltpu.make_async_remote_copy(
            src_ref=source,
            dst_ref=held.at[(d + 2) * heads + h],
            send_sem=up_sem.at[d * heads + h],
            recv_sem=recv_sem.at[(d + 2) * heads + h],
            device_id={"sp": me + 2},
            device_id_type=MESH,
        )

    def side(d, h, slot, source):
        return pltpu.make_async_remote_copy(
            src_ref=source,
            dst_ref=held.at[slot * heads + h],
            send_sem=side_sem.at[d * heads + h],
            recv_sem=recv_sem.at[slot * heads + h],
            device_id={"sp": partner},
            device_id_type=MESH,
        )

    def send(d, h, source):
        pl.when(has_up)(lambda: up(d, h, source).start())
        pl.when(odd == 0)(lambda: side(d, h, d + 1, source).start())
        pl.when((odd == 1) & (d >= 2))(lambda: side(d, h, d - 1, source).start())

    def sent(d, h, source):
        pl.when(has_up)(lambda: up(d, h, source).wait_send())
        pl.when(odd == 0)(lambda: side(d, h, d + 1, source).wait_send())
        pl.when((odd == 1) & (d >= 2))(lambda: side(d, h, d - 1, source).wait_send())

    def arrived(d, h):
        pltpu.make_async_remote_copy(
            src_ref=held.at[d * heads + h],
            dst_ref=held.at[d * heads + h],
            send_sem=up_sem.at[d * heads + h],
            recv_sem=recv_sem.at[d * heads + h],
            device_id={"sp": partner},
            device_id_type=MESH,
        ).wait_recv()

    per_block = BLOCK // PAIR

    def attend_rows(sources, q0, todo, masked):
        rows = pl.ds(q0, QUERY_ROWS)
        units = [(h, block) for block in todo for h in range(heads)]
        rest, soft, beyond = {}, {}, {}
        earlier = None
        if masked is not None:
            earlier = lax.broadcasted_iota(
                jnp.int32, (QUERY_ROWS, BLOCK), 1
            ) < lax.broadcasted_iota(jnp.int32, (QUERY_ROWS, BLOCK), 0)
        for h, block in units:
            b0 = block * BLOCK
            bias = sources[h][length : length + BIAS_ROWS, :].astype(jnp.float32)
            bias_row = jnp.concatenate(
                [
                    bias[block * per_block + i : block * per_block + i + 1]
                    for i in range(per_block)
                ],
                axis=1,
            )
            scores = lax.dot_general(
                q_ref[h, rows, :],
                sources[h][b0 : b0 + BLOCK, :],
                (((1,), (1,)), ((), ())),
                preferred_element_type=jnp.float32,
            )
            scores = scores + bias_row
            value = jnp.maximum(scores, 0.0) + jnp.log(1.0 + jnp.exp(-jnp.abs(scores)))
            rest[h, block] = scores - value
            if block == masked:
                value = jnp.where(earlier, value, 0.0)
            soft[h, block] = value
            beyond[h, block] = jnp.dot(
                value.astype(jnp.bfloat16), tri[...], preferred_element_type=jnp.float32
            )
        for h in range(heads):
            later = after[h, rows, :]
            gathered = total[h, rows, :]
            for block in todo:
                b0 = block * BLOCK
                past = beyond[h, block]
                piece = jnp.exp(rest[h, block] - past - jnp.concatenate([later] * per_block, axis=1))
                if block == masked:
                    piece = jnp.where(earlier, piece, 0.0)
                gathered = gathered + jnp.dot(
                    piece.astype(jnp.bfloat16),
                    sources[h][b0 : b0 + BLOCK, :],
                    preferred_element_type=jnp.float32,
                )
                later = later + (past[:, :1] + soft[h, block][:, :1])
            total[h, rows, :] = gathered
            after[h, rows, :] = later

    blocks = length // BLOCK

    def compute_own():
        sources = [own_ref.at[h] for h in range(heads)]
        for c in range(blocks):
            attend_rows(sources, c * BLOCK, list(reversed(range(c + 1))), c)

    def compute(d):
        sources = [held.at[d * heads + h] for h in range(heads)]

        def chunk(c, carry):
            q0 = pl.multiple_of(c * QUERY_ROWS, QUERY_ROWS)
            attend_rows(sources, q0, list(reversed(range(blocks))), None)
            return carry

        lax.fori_loop(0, length // QUERY_ROWS, chunk, 0)

    for h in range(heads):
        send(0, h, own_ref.at[h])
    compute_own()

    def step(k, carry):
        @pl.when(k <= level)
        def _():
            for h in range(heads):
                arrived(2 * k, h)
                send(2 * k, h, held.at[2 * k * heads + h])

        first = 2 * k - 3 + 2 * odd

        @pl.when(first >= 1)
        def _():
            for h in range(heads):
                arrived(first, h)

        def one(d, inner):
            compute(d)
            return inner

        lax.fori_loop(jnp.maximum(first, 1), jnp.minimum(first + 1, me) + 1, one, 0)
        return carry

    lax.fori_loop(1, level + 2, step, 0)
    for load in loads:
        load.start()
    lane = lax.broadcasted_iota(jnp.int32, (length, PAIR), 1)
    for h in range(0, heads, 2):
        joined = total[h]
        if h + 1 < heads:
            joined = jnp.where(lane >= HEAD_DIM, total[h + 1], joined)
        columns = min(PAIR, (heads - h) * HEAD_DIM)
        attended[:, h * HEAD_DIM : h * HEAD_DIM + columns] = joined[:, :columns].astype(jnp.bfloat16)


    tokens, width_model = residual.shape

    def share(k):
        target = lax.rem(my_t + k, groups)
        return pltpu.make_async_remote_copy(
            src_ref=attended.at[pl.ds(pl.multiple_of(target * tokens, tokens), tokens)],
            dst_ref=heads_in.at[my_t],
            send_sem=share_send.at[k],
            recv_sem=share_recv.at[my_t],
            device_id={"tp": target},
            device_id_type=MESH,
        )

    def shared(t):
        pltpu.make_async_remote_copy(
            src_ref=heads_in.at[t],
            dst_ref=heads_in.at[t],
            send_sem=share_send.at[0],
            recv_sem=share_recv.at[t],
            device_id={"tp": mate},
            device_id_type=MESH,
        ).wait_recv()

    for k in range(1, groups):
        share(k).start()
    heads_in[my_t] = attended[pl.ds(pl.multiple_of(my_t * tokens, tokens), tokens)]
    for k in range(1, groups):
        shared(lax.rem(my_t + k, groups))
    token_heads = jnp.concatenate([heads_in[t] for t in range(groups)], axis=1)
    squares = jnp.zeros((tokens, 1), jnp.float32)
    wide = min(WIDE, width_model)
    for first in range(0, width_model, wide):
        columns = slice(first, first + wide)
        projected = jnp.dot(token_heads, out_weight[:, columns], preferred_element_type=jnp.float32)
        piece = (residual[:, columns].astype(jnp.float32) + projected).astype(jnp.bfloat16)
        mixed[:, columns] = piece
        piece = piece.astype(jnp.float32)
        squares = squares + jnp.sum(piece * piece, axis=1, keepdims=True)
    scale = lax.rsqrt(squares / width_model + epsilon)
    capacity = outgoing.shape[1]
    for first in range(0, width_model, wide):
        columns = slice(first, first + wide)
        piece = mixed[:, columns].astype(jnp.float32) * scale * gain[:, columns]
        placed = jnp.dot(place[...], piece.astype(jnp.bfloat16), preferred_element_type=jnp.float32)
        for e in range(n):
            outgoing[e, :, columns] = placed[e * capacity : (e + 1) * capacity].astype(jnp.bfloat16)

    def copy(source, t, s, send_sem, device):
        return pltpu.make_async_remote_copy(
            src_ref=source,
            dst_ref=rows.at[t * n + s],
            send_sem=send_sem,
            recv_sem=row_sem.at[t * n + s],
            device_id=device,
            device_id_type=MESH,
        )

    def to_expert(r):
        target = lax.rem(me + r, n)
        return copy(outgoing.at[target], my_t, me, sp_sem.at[r], {"sp": target})

    def to_chip(k, s, source):
        return copy(source, my_t, s, chip_sem.at[k * n + s], {"tp": alike[k]})

    def to_mate(t, s, source):
        return copy(source, t, s, core_sem.at[t * n + s], {"tp": mate})

    def row_arrived(t, s):
        copy(rows.at[t * n + s], t, s, core_sem.at[t * n + s], {"tp": mate}).wait_recv()

    def spread(s, source):
        for k in range(chips - 1):
            to_chip(k, s, source).start()
        to_mate(my_t, s, source).start()

    def issue(r, carry):
        to_expert(r).start()
        return carry

    spread(me, outgoing.at[me])
    lax.fori_loop(1, n, issue, 0)
    rows[my_t * n + me] = outgoing[me]
    for load in loads:
        load.wait()

    def source_of(j):
        return lax.rem(me + n - j, n)

    def take(j):
        s = source_of(j)

        @pl.when(s != me)
        def _():
            row_arrived(my_t, s)
            spread(s, rows.at[my_t * n + s])

    def relay(j):
        s = source_of(j)
        for t in alike:
            row_arrived(t, s)
            to_mate(t, s, rows.at[t * n + s]).start()

    def expert(j):
        s = source_of(j)
        row_arrived(mate, s)
        for t in alike:
            row_arrived(t + 1 - 2 * lax.rem(t, 2), s)
        block[...] = jnp.concatenate([rows[t * n + s] for t in range(groups)], axis=0)
        unit_step = min(UNITS, gate.shape[1])

        def units(f, carry):
            columns = pl.ds(pl.multiple_of(f * unit_step, unit_step), unit_step)
            gate_act = jnp.dot(block[...], gate[:, columns], preferred_element_type=jnp.float32)
            up_act = jnp.dot(block[...], up_w[:, columns], preferred_element_type=jnp.float32)
            silu = gate_act / (1.0 + jnp.exp(-gate_act))
            hidden[:, columns] = (silu * up_act).astype(jnp.bfloat16)
            return carry

        lax.fori_loop(0, gate.shape[1] // unit_step, units, 0)
        step = min(FEATURES, width_model)

        def features(f, carry):
            columns = pl.ds(pl.multiple_of(f * step, step), step)
            value = jnp.dot(hidden[...], down[:, columns], preferred_element_type=jnp.float32)
            for t in range(groups):
                piece = value[t * capacity : (t + 1) * capacity]
                partial[t * n + s, :, columns] = piece.astype(jnp.bfloat16)
            return carry

        lax.fori_loop(0, width_model // step, features, 0)
        for chip in range(chips):
            pair_copy(chip, j).start()

    def pair_copy(chip, j):
        return pltpu.make_async_remote_copy(
            src_ref=partial.at[(2 * chip + 1 - core) * n + source_of(j)],
            dst_ref=pair.at[chip * n + j],
            send_sem=pair_send.at[chip * n + j],
            recv_sem=pair_recv.at[chip * n + j],
            device_id={"tp": mate},
            device_id_type=MESH,
        )

    def chip_copy(k, j):
        return pltpu.make_async_remote_copy(
            src_ref=pair.at[(alike[k] // 2) * n + j],
            dst_ref=other.at[k * n + j],
            send_sem=chip_send.at[k * n + j],
            recv_sem=chip_recv.at[k * n + j],
            device_id={"tp": alike[k]},
            device_id_type=MESH,
        )

    def back_copy(j):
        return pltpu.make_async_remote_copy(
            src_ref=done.at[j],
            dst_ref=back.at[me],
            send_sem=back_send.at[j],
            recv_sem=back_recv.at[me],
            device_id={"sp": source_of(j)},
            device_id_type=MESH,
        )

    def sum_pairs(j):
        for chip in range(chips):
            pair_copy(chip, j).wait_recv()
        for k in range(chips - 1):
            chip = alike[k] // 2
            pair[chip * n + j] = (
                partial[alike[k] * n + source_of(j)].astype(jnp.float32)
                + pair[chip * n + j].astype(jnp.float32)
            ).astype(jnp.bfloat16)
        for k in range(chips - 1):
            chip_copy(k, j).start()

    def give_back(j):
        s = source_of(j)
        value = partial[my_t * n + s].astype(jnp.float32) + pair[(my_t // 2) * n + j].astype(
            jnp.float32
        )
        for k in range(chips - 1):
            chip_copy(k, j).wait_recv()
            value = value + other[k * n + j].astype(jnp.float32)
        value = value.astype(jnp.bfloat16)

        @pl.when(s == me)
        def _():
            back[me] = value

        @pl.when(s != me)
        def _():
            done[j] = value
            back_copy(j).start()

    def flow(j, carry):
        pl.when((j >= 4) & (j < n + 4))(lambda: give_back(j - 4))
        pl.when((j >= 3) & (j < n + 3))(lambda: sum_pairs(j - 3))
        pl.when((j >= 2) & (j < n + 2))(lambda: expert(j - 2))
        pl.when(j < n)(lambda: take(j))
        pl.when((j >= 1) & (j < n + 1))(lambda: relay(j - 1))
        return carry

    lax.fori_loop(0, n + 4, flow, 0)

    for h in range(heads):
        sent(0, h, own_ref.at[h])

    def drain(k, carry):
        for h in range(heads):
            sent(2 * k, h, held.at[2 * k * heads + h])
        return carry

    lax.fori_loop(1, level + 1, drain, 0)

    for k in range(1, groups):
        share(k).wait_send()

    def finish(j, carry):
        s = source_of(j)
        pl.when(j >= 1)(lambda: to_expert(j).wait_send())
        for k in range(chips - 1):
            to_chip(k, s, outgoing.at[me]).wait_send()
            to_mate(alike[k], s, outgoing.at[me]).wait_send()
            chip_copy(k, j).wait_send()
        to_mate(my_t, s, outgoing.at[me]).wait_send()
        for chip in range(chips):
            pair_copy(chip, j).wait_send()

        @pl.when(s != me)
        def _():
            back_copy(j).wait_send()
            pltpu.make_async_remote_copy(
                src_ref=done.at[j],
                dst_ref=back.at[s],
                send_sem=back_send.at[j],
                recv_sem=back_recv.at[s],
                device_id={"sp": s},
                device_id_type=MESH,
            ).wait_recv()

        return carry

    lax.fori_loop(0, n, finish, 0)


def greet_all(n, groups, me, my_t):
    barrier = pltpu.get_barrier_semaphore()

    def greet(device):
        pl.semaphore_signal(barrier, inc=1, device_id=device, device_id_type=MESH)

    def greet_sp(r, carry):
        greet({"sp": lax.rem(me + r, n)})
        return carry

    lax.fori_loop(1, n, greet_sp, 0)
    for k in range(1, groups):
        greet({"tp": lax.rem(my_t + k, groups)})
    pl.semaphore_wait(barrier, n - 1 + groups - 1)


def layer(queries, keys, values, key_bias, place, residual, out_weight, gain, gate, up, down):
    n, groups = lax.axis_size("sp"), lax.axis_size("tp")
    chips = groups // 2
    length = queries.shape[0]
    heads = key_bias.shape[1]
    width = heads * HEAD_DIM
    tokens, width_model = residual.shape
    capacity = place.shape[0] // n
    units = gate.shape[1]
    apart = max(1, chips - 1) * n
    scaled = queries * jnp.bfloat16(HEAD_DIM ** (-0.5))
    bias_rows = jnp.transpose(key_bias).reshape(heads, -1, PAIR)
    bias_rows = jnp.pad(bias_rows, ((0, 0), (0, BIAS_ROWS - bias_rows.shape[1]), (0, 0)))
    nothing = jnp.zeros((length, HEAD_DIM), queries.dtype)
    per_head, own = [], []
    for h in range(heads):
        columns = slice(h * HEAD_DIM, (h + 1) * HEAD_DIM)
        order = 1 if h % 2 == 0 else -1
        per_head.append(jnp.concatenate([nothing, scaled[:, columns]][::order], axis=1))
        own.append(jnp.concatenate([values[:, columns], keys[:, columns]][::order], axis=1))
    own = jnp.concatenate([jnp.stack(own), bias_rows], axis=1)
    vmem = pl.BlockSpec(memory_space=pltpu.VMEM)
    anywhere = pl.BlockSpec(memory_space=pl.ANY)
    kind = queries.dtype
    return pl.pallas_call(
        functools.partial(layer_kernel, n, groups, length, heads),
        out_shape=(
            jax.ShapeDtypeStruct((n, capacity, width_model), kind),
            jax.ShapeDtypeStruct((tokens, width_model), kind),
        ),
        in_specs=[vmem] * 6 + [anywhere] * 3,
        out_specs=(vmem, vmem),
        scratch_shapes=[
            pltpu.VMEM(((n + 1) * heads, length + BIAS_ROWS, PAIR), kind),
            pltpu.VMEM((heads, length, PAIR), jnp.float32),
            pltpu.VMEM((heads, length, PAIR), jnp.float32),
            pltpu.VMEM((BLOCK, BLOCK), kind),
            pltpu.VMEM((length, width), kind),
            pltpu.VMEM((groups, tokens, width), kind),
            pltpu.VMEM((n, capacity, width_model), kind),
            pltpu.VMEM((groups * n, capacity, width_model), kind),
            pltpu.VMEM((groups * n, capacity, width_model), kind),
            pltpu.VMEM((groups * capacity, width_model), kind),
            pltpu.VMEM((groups * capacity, units), kind),
            pltpu.VMEM((width_model, units), kind),
            pltpu.VMEM((width_model, units), kind),
            pltpu.VMEM((units, width_model), kind),
            pltpu.VMEM((chips * n, capacity, width_model), kind),
            pltpu.VMEM((apart, capacity, width_model), kind),
            pltpu.VMEM((n, capacity, width_model), kind),
            pltpu.SemaphoreType.DMA(((n + 2) * heads,)),
            pltpu.SemaphoreType.DMA(((n + 2) * heads,)),
            pltpu.SemaphoreType.DMA(((n + 2) * heads,)),
            pltpu.SemaphoreType.DMA((groups,)),
            pltpu.SemaphoreType.DMA((groups,)),
            pltpu.SemaphoreType.DMA((3,)),
            pltpu.SemaphoreType.DMA((n,)),
            pltpu.SemaphoreType.DMA((apart,)),
            pltpu.SemaphoreType.DMA((groups * n,)),
            pltpu.SemaphoreType.DMA((groups * n,)),
            pltpu.SemaphoreType.DMA((chips * n,)),
            pltpu.SemaphoreType.DMA((chips * n,)),
            pltpu.SemaphoreType.DMA((apart,)),
            pltpu.SemaphoreType.DMA((apart,)),
            pltpu.SemaphoreType.DMA((n,)),
            pltpu.SemaphoreType.DMA((n,)),
        ],
        compiler_params=pltpu.CompilerParams(
            collective_id=0, has_side_effects=True, vmem_limit_bytes=62 * 1024 * 1024
        ),
        name="layer",
    )(jnp.stack(per_head), own, place, residual, out_weight, gain, gate, up, down)


def shards(
    queries,
    keys,
    values,
    key_bias,
    residual,
    out_weight,
    norm_gain,
    routes,
    route_weights,
    gate_weight,
    up_weight,
    down_weight,
):
    sp_count = lax.axis_size("sp")
    token_count = residual.shape[0]
    width_model = residual.shape[1]
    capacity = max(2, 5 * token_count * TOP // (4 * sp_count))
    flat_routes = routes.reshape(-1)
    onehot = (flat_routes[:, None] == lax.iota(jnp.int32, sp_count)[None, :]).astype(jnp.int32)
    before = jnp.cumsum(onehot, axis=0) - onehot
    slot_of = flat_routes * capacity + jnp.sum(before * onehot, axis=1)
    select = (slot_of[:, None] == lax.iota(jnp.int32, sp_count * capacity)[None, :]).astype(
        jnp.bfloat16
    )
    placing = jnp.sum(select.reshape(token_count, TOP, sp_count * capacity), axis=1)
    returned, mixed = layer(
        queries, keys, values, key_bias, jnp.transpose(placing), residual, out_weight,
        norm_gain[None, :], gate_weight[0], up_weight[0], down_weight[0],
    )
    returned = returned.reshape(-1, width_model)
    picked = jnp.dot(select, returned, preferred_element_type=jnp.float32).reshape(
        token_count, TOP, width_model
    )
    routed = jnp.sum(picked * route_weights[:, :, None], axis=1)
    return (mixed.astype(jnp.float32) + routed).astype(jnp.bfloat16)


def solution(mesh):
    return jax.shard_map(
        shards,
        mesh=mesh,
        in_specs=(
            P("sp", "tp"),
            P("sp", "tp"),
            P("sp", "tp"),
            P("sp", "tp"),
            P(("sp", "tp"), None),
            P(),
            P(),
            P(("sp", "tp"), None),
            P(("sp", "tp"), None),
            P("sp", None, "tp"),
            P("sp", None, "tp"),
            P("sp", "tp", None),
        ),
        out_specs=P(("sp", "tp"), None),
        check_vma=False,
    )
```

```python
import functools

import jax
import jax.numpy as jnp
from jax import lax
from jax.experimental import pallas as pl
from jax.experimental.pallas import tpu as pltpu
from jax.sharding import PartitionSpec as P

HEAD_DIM = 64
TOP = 2
SPAN = 512
BLOCK = 256
QUERY_ROWS = 256
BIAS_ROWS = 16
PAIR = 2 * HEAD_DIM
WIDE = 512
UNITS = 512
FEATURES = 1024
MESH = pl.DeviceIdType.MESH


epsilon = 1e-06


def layer_kernel(
    n, groups, length, heads,
    queries, keys, values, bias, routes, route_weights, residual, out_weight, gain,
    gate_hbm, up_hbm, down_hbm, out,
    q_ref, own_ref, place, back, mixed, held, total, after, tri, attended, heads_in, outgoing, rows, partial, block, hidden,
    gate, up_w, down, pair, other, done,
    up_sem, side_sem, recv_sem, share_send, share_recv, weight_sem, sp_sem, chip_sem, core_sem,
    row_sem, pair_send, pair_recv, chip_send, chip_recv, back_send, back_recv,
):
    me, my_t = lax.axis_index("sp"), lax.axis_index("tp")
    odd = lax.rem(me, 2)
    level = me // 2
    partner = me + 1 - 2 * odd
    has_up = me + 2 < n
    core = lax.rem(my_t, 2)
    mate = my_t + 1 - 2 * core
    chips = groups // 2
    alike = [lax.rem(my_t + 2 * k, groups) for k in range(1, chips)]
    loads = [
        pltpu.make_async_copy(gate_hbm, gate, weight_sem.at[0]),
        pltpu.make_async_copy(up_hbm, up_w, weight_sem.at[1]),
        pltpu.make_async_copy(down_hbm, down, weight_sem.at[2]),
    ]
    greet_all(n, groups, me, my_t)
    build_heads(length, heads, queries, keys, values, bias, q_ref, own_ref)
    capacity = outgoing.shape[1]
    slots = slots_of(n, capacity, routes)
    for first in range(0, n * capacity, 64):
        slot = first + lax.broadcasted_iota(jnp.int32, (64, routes.shape[1]), 0)
        hit = jnp.zeros(slot.shape, jnp.float32)
        for row in slots:
            hit = hit + (slot == row).astype(jnp.float32)
        place[first : first + 64, :] = hit.astype(jnp.bfloat16)
    total[...] = jnp.zeros_like(total)
    after[...] = jnp.zeros_like(after)
    tri_row = lax.broadcasted_iota(jnp.int32, (BLOCK, BLOCK), 0)
    tri_col = lax.broadcasted_iota(jnp.int32, (BLOCK, BLOCK), 1)
    tri[...] = (tri_row > tri_col).astype(jnp.float32).astype(jnp.bfloat16)
    pl.semaphore_wait(pltpu.get_barrier_semaphore(), n - 1 + groups - 1)

    def up(d, h, source):
        return pltpu.make_async_remote_copy(
            src_ref=source,
            dst_ref=held.at[(d + 2) * heads + h],
            send_sem=up_sem.at[d * heads + h],
            recv_sem=recv_sem.at[(d + 2) * heads + h],
            device_id={"sp": me + 2},
            device_id_type=MESH,
        )

    def side(d, h, slot, source):
        return pltpu.make_async_remote_copy(
            src_ref=source,
            dst_ref=held.at[slot * heads + h],
            send_sem=side_sem.at[d * heads + h],
            recv_sem=recv_sem.at[slot * heads + h],
            device_id={"sp": partner},
            device_id_type=MESH,
        )

    def send(d, h, source):
        pl.when(has_up)(lambda: up(d, h, source).start())
        pl.when(odd == 0)(lambda: side(d, h, d + 1, source).start())
        pl.when((odd == 1) & (d >= 2))(lambda: side(d, h, d - 1, source).start())

    def sent(d, h, source):
        pl.when(has_up)(lambda: up(d, h, source).wait_send())
        pl.when(odd == 0)(lambda: side(d, h, d + 1, source).wait_send())
        pl.when((odd == 1) & (d >= 2))(lambda: side(d, h, d - 1, source).wait_send())

    def arrived(d, h):
        pltpu.make_async_remote_copy(
            src_ref=held.at[d * heads + h],
            dst_ref=held.at[d * heads + h],
            send_sem=up_sem.at[d * heads + h],
            recv_sem=recv_sem.at[d * heads + h],
            device_id={"sp": partner},
            device_id_type=MESH,
        ).wait_recv()

    per_block = BLOCK // PAIR

    def attend_rows(sources, q0, todo, masked):
        rows = pl.ds(q0, QUERY_ROWS)
        units = [(h, block) for block in todo for h in range(heads)]
        rest, soft, beyond = {}, {}, {}
        earlier = None
        if masked is not None:
            earlier = lax.broadcasted_iota(
                jnp.int32, (QUERY_ROWS, BLOCK), 1
            ) < lax.broadcasted_iota(jnp.int32, (QUERY_ROWS, BLOCK), 0)
        for h, block in units:
            b0 = block * BLOCK
            bias = sources[h][length : length + BIAS_ROWS, :].astype(jnp.float32)
            bias_row = jnp.concatenate(
                [
                    bias[block * per_block + i : block * per_block + i + 1]
                    for i in range(per_block)
                ],
                axis=1,
            )
            scores = lax.dot_general(
                q_ref[h, rows, :],
                sources[h][b0 : b0 + BLOCK, :],
                (((1,), (1,)), ((), ())),
                preferred_element_type=jnp.float32,
            )
            scores = scores + bias_row
            value = jnp.maximum(scores, 0.0) + jnp.log(1.0 + jnp.exp(-jnp.abs(scores)))
            rest[h, block] = scores - value
            if block == masked:
                value = jnp.where(earlier, value, 0.0)
            soft[h, block] = value
            beyond[h, block] = jnp.dot(
                value.astype(jnp.bfloat16), tri[...], preferred_element_type=jnp.float32
            )
        for h in range(heads):
            later = after[h, rows, :]
            gathered = total[h, rows, :]
            for block in todo:
                b0 = block * BLOCK
                past = beyond[h, block]
                piece = jnp.exp(rest[h, block] - past - jnp.concatenate([later] * per_block, axis=1))
                if block == masked:
                    piece = jnp.where(earlier, piece, 0.0)
                gathered = gathered + jnp.dot(
                    piece.astype(jnp.bfloat16),
                    sources[h][b0 : b0 + BLOCK, :],
                    preferred_element_type=jnp.float32,
                )
                later = later + (past[:, :1] + soft[h, block][:, :1])
            total[h, rows, :] = gathered
            after[h, rows, :] = later

    blocks = length // BLOCK

    def compute_own():
        sources = [own_ref.at[h] for h in range(heads)]
        for c in range(blocks):
            attend_rows(sources, c * BLOCK, list(reversed(range(c + 1))), c)

    def compute(d):
        sources = [held.at[d * heads + h] for h in range(heads)]

        def chunk(c, carry):
            q0 = pl.multiple_of(c * QUERY_ROWS, QUERY_ROWS)
            attend_rows(sources, q0, list(reversed(range(blocks))), None)
            return carry

        lax.fori_loop(0, length // QUERY_ROWS, chunk, 0)

    for h in range(heads):
        send(0, h, own_ref.at[h])
    compute_own()

    def step(k, carry):
        @pl.when(k <= level)
        def _():
            for h in range(heads):
                arrived(2 * k, h)
                send(2 * k, h, held.at[2 * k * heads + h])

        first = 2 * k - 3 + 2 * odd

        @pl.when(first >= 1)
        def _():
            for h in range(heads):
                arrived(first, h)

        def one(d, inner):
            compute(d)
            return inner

        lax.fori_loop(jnp.maximum(first, 1), jnp.minimum(first + 1, me) + 1, one, 0)
        return carry

    lax.fori_loop(1, level + 2, step, 0)
    for load in loads:
        load.start()
    lane = lax.broadcasted_iota(jnp.int32, (length, PAIR), 1)
    for h in range(0, heads, 2):
        joined = total[h]
        if h + 1 < heads:
            joined = jnp.where(lane >= HEAD_DIM, total[h + 1], joined)
        columns = min(PAIR, (heads - h) * HEAD_DIM)
        attended[:, h * HEAD_DIM : h * HEAD_DIM + columns] = joined[:, :columns].astype(jnp.bfloat16)


    tokens, width_model = residual.shape

    def share(k):
        target = lax.rem(my_t + k, groups)
        return pltpu.make_async_remote_copy(
            src_ref=attended.at[pl.ds(pl.multiple_of(target * tokens, tokens), tokens)],
            dst_ref=heads_in.at[my_t],
            send_sem=share_send.at[k],
            recv_sem=share_recv.at[my_t],
            device_id={"tp": target},
            device_id_type=MESH,
        )

    def shared(t):
        pltpu.make_async_remote_copy(
            src_ref=heads_in.at[t],
            dst_ref=heads_in.at[t],
            send_sem=share_send.at[0],
            recv_sem=share_recv.at[t],
            device_id={"tp": mate},
            device_id_type=MESH,
        ).wait_recv()

    for k in range(1, groups):
        share(k).start()
    heads_in[my_t] = attended[pl.ds(pl.multiple_of(my_t * tokens, tokens), tokens)]
    for k in range(1, groups):
        shared(lax.rem(my_t + k, groups))
    token_heads = jnp.concatenate([heads_in[t] for t in range(groups)], axis=1)
    squares = jnp.zeros((tokens, 1), jnp.float32)
    wide = min(WIDE, width_model)
    for first in range(0, width_model, wide):
        columns = slice(first, first + wide)
        projected = jnp.dot(token_heads, out_weight[:, columns], preferred_element_type=jnp.float32)
        piece = (residual[:, columns].astype(jnp.float32) + projected).astype(jnp.bfloat16)
        mixed[:, columns] = piece
        piece = piece.astype(jnp.float32)
        squares = squares + jnp.sum(piece * piece, axis=1, keepdims=True)
    scale = lax.rsqrt(squares / width_model + epsilon)
    for first in range(0, width_model, wide):
        columns = slice(first, first + wide)
        piece = mixed[:, columns].astype(jnp.float32) * scale * gain[:, columns]
        placed = jnp.dot(place[...], piece.astype(jnp.bfloat16), preferred_element_type=jnp.float32)
        for e in range(n):
            outgoing[e, :, columns] = placed[e * capacity : (e + 1) * capacity].astype(jnp.bfloat16)

    def copy(source, t, s, send_sem, device):
        return pltpu.make_async_remote_copy(
            src_ref=source,
            dst_ref=rows.at[t * n + s],
            send_sem=send_sem,
            recv_sem=row_sem.at[t * n + s],
            device_id=device,
            device_id_type=MESH,
        )

    def to_expert(r):
        target = lax.rem(me + r, n)
        return copy(outgoing.at[target], my_t, me, sp_sem.at[r], {"sp": target})

    def to_chip(k, s, source):
        return copy(source, my_t, s, chip_sem.at[k * n + s], {"tp": alike[k]})

    def to_mate(t, s, source):
        return copy(source, t, s, core_sem.at[t * n + s], {"tp": mate})

    def row_arrived(t, s):
        copy(rows.at[t * n + s], t, s, core_sem.at[t * n + s], {"tp": mate}).wait_recv()

    def spread(s, source):
        for k in range(chips - 1):
            to_chip(k, s, source).start()
        to_mate(my_t, s, source).start()

    def issue(r, carry):
        to_expert(r).start()
        return carry

    spread(me, outgoing.at[me])
    lax.fori_loop(1, n, issue, 0)
    rows[my_t * n + me] = outgoing[me]
    for load in loads:
        load.wait()

    def source_of(j):
        return lax.rem(me + n - j, n)

    def take(j):
        s = source_of(j)

        @pl.when(s != me)
        def _():
            row_arrived(my_t, s)
            spread(s, rows.at[my_t * n + s])

    def relay(j):
        s = source_of(j)
        for t in alike:
            row_arrived(t, s)
            to_mate(t, s, rows.at[t * n + s]).start()

    def expert(j):
        s = source_of(j)
        row_arrived(mate, s)
        for t in alike:
            row_arrived(t + 1 - 2 * lax.rem(t, 2), s)
        block[...] = jnp.concatenate([rows[t * n + s] for t in range(groups)], axis=0)
        unit_step = min(UNITS, gate.shape[1])

        def units(f, carry):
            columns = pl.ds(pl.multiple_of(f * unit_step, unit_step), unit_step)
            gate_act = jnp.dot(block[...], gate[:, columns], preferred_element_type=jnp.float32)
            up_act = jnp.dot(block[...], up_w[:, columns], preferred_element_type=jnp.float32)
            silu = gate_act / (1.0 + jnp.exp(-gate_act))
            hidden[:, columns] = (silu * up_act).astype(jnp.bfloat16)
            return carry

        lax.fori_loop(0, gate.shape[1] // unit_step, units, 0)
        step = min(FEATURES, width_model)

        def features(f, carry):
            columns = pl.ds(pl.multiple_of(f * step, step), step)
            value = jnp.dot(hidden[...], down[:, columns], preferred_element_type=jnp.float32)
            for t in range(groups):
                piece = value[t * capacity : (t + 1) * capacity]
                partial[t * n + s, :, columns] = piece.astype(jnp.bfloat16)
            return carry

        lax.fori_loop(0, width_model // step, features, 0)
        for chip in range(chips):
            pair_copy(chip, j).start()

    def pair_copy(chip, j):
        return pltpu.make_async_remote_copy(
            src_ref=partial.at[(2 * chip + 1 - core) * n + source_of(j)],
            dst_ref=pair.at[chip * n + j],
            send_sem=pair_send.at[chip * n + j],
            recv_sem=pair_recv.at[chip * n + j],
            device_id={"tp": mate},
            device_id_type=MESH,
        )

    def chip_copy(k, j):
        return pltpu.make_async_remote_copy(
            src_ref=pair.at[(alike[k] // 2) * n + j],
            dst_ref=other.at[k * n + j],
            send_sem=chip_send.at[k * n + j],
            recv_sem=chip_recv.at[k * n + j],
            device_id={"tp": alike[k]},
            device_id_type=MESH,
        )

    def back_copy(j):
        return pltpu.make_async_remote_copy(
            src_ref=done.at[j],
            dst_ref=back.at[me],
            send_sem=back_send.at[j],
            recv_sem=back_recv.at[me],
            device_id={"sp": source_of(j)},
            device_id_type=MESH,
        )

    def sum_pairs(j):
        for chip in range(chips):
            pair_copy(chip, j).wait_recv()
        for k in range(chips - 1):
            chip = alike[k] // 2
            pair[chip * n + j] = (
                partial[alike[k] * n + source_of(j)].astype(jnp.float32)
                + pair[chip * n + j].astype(jnp.float32)
            ).astype(jnp.bfloat16)
        for k in range(chips - 1):
            chip_copy(k, j).start()

    def give_back(j):
        s = source_of(j)
        value = partial[my_t * n + s].astype(jnp.float32) + pair[(my_t // 2) * n + j].astype(
            jnp.float32
        )
        for k in range(chips - 1):
            chip_copy(k, j).wait_recv()
            value = value + other[k * n + j].astype(jnp.float32)
        value = value.astype(jnp.bfloat16)

        @pl.when(s == me)
        def _():
            back[me] = value

        @pl.when(s != me)
        def _():
            done[j] = value
            back_copy(j).start()

    def flow(j, carry):
        pl.when((j >= 4) & (j < n + 4))(lambda: give_back(j - 4))
        pl.when((j >= 3) & (j < n + 3))(lambda: sum_pairs(j - 3))
        pl.when((j >= 2) & (j < n + 2))(lambda: expert(j - 2))
        pl.when(j < n)(lambda: take(j))
        pl.when((j >= 1) & (j < n + 1))(lambda: relay(j - 1))
        return carry

    lax.fori_loop(0, n + 4, flow, 0)

    for h in range(heads):
        sent(0, h, own_ref.at[h])

    def drain(k, carry):
        for h in range(heads):
            sent(2 * k, h, held.at[2 * k * heads + h])
        return carry

    lax.fori_loop(1, level + 1, drain, 0)

    for k in range(1, groups):
        share(k).wait_send()

    def finish(j, carry):
        s = source_of(j)
        pl.when(j >= 1)(lambda: to_expert(j).wait_send())
        for k in range(chips - 1):
            to_chip(k, s, outgoing.at[me]).wait_send()
            to_mate(alike[k], s, outgoing.at[me]).wait_send()
            chip_copy(k, j).wait_send()
        to_mate(my_t, s, outgoing.at[me]).wait_send()
        for chip in range(chips):
            pair_copy(chip, j).wait_send()

        @pl.when(s != me)
        def _():
            back_copy(j).wait_send()
            pltpu.make_async_remote_copy(
                src_ref=done.at[j],
                dst_ref=back.at[s],
                send_sem=back_send.at[j],
                recv_sem=back_recv.at[s],
                device_id={"sp": s},
                device_id_type=MESH,
            ).wait_recv()

        return carry

    lax.fori_loop(0, n, finish, 0)
    extra = [row.astype(jnp.float32) for row in slots]
    extra += [route_weights[k : k + 1, :] for k in range(TOP)]
    extra += [jnp.zeros((8 - len(extra), tokens), jnp.float32)]
    across = jnp.transpose(jnp.concatenate(extra, axis=0))
    slot = lax.broadcasted_iota(jnp.int32, (tokens, n * capacity), 1)
    select = [
        (slot == across[:, k : k + 1].astype(jnp.int32)).astype(jnp.float32).astype(jnp.bfloat16)
        for k in range(TOP)
    ]
    for first in range(0, width_model, wide):
        columns = slice(first, first + wide)
        returned = jnp.concatenate([back[e, :, columns] for e in range(n)], axis=0)
        value = mixed[:, columns].astype(jnp.float32)
        routed = jnp.zeros((tokens, wide), jnp.float32)
        for k in range(TOP):
            picked = jnp.dot(select[k], returned, preferred_element_type=jnp.float32)
            routed = routed + picked * across[:, TOP + k : TOP + k + 1]
        out[:, columns] = (value + routed).astype(out.dtype)


def build_heads(length, heads, queries, keys, values, bias, q_ref, own_ref):
    for h in range(heads):
        columns = slice(h * HEAD_DIM, (h + 1) * HEAD_DIM)
        order = 1 if h % 2 == 0 else -1
        for first in range(0, length, 256):
            rows = slice(first, first + 256)
            query = queries[rows, columns].astype(jnp.float32) * HEAD_DIM ** (-0.5)
            parts = [jnp.zeros_like(query), query][::order]
            q_ref[h, rows, :] = jnp.concatenate(parts, axis=1).astype(jnp.bfloat16)
            parts = [values[rows, columns], keys[rows, columns]][::order]
            parts = [part.astype(jnp.float32) for part in parts]
            own_ref[h, rows, :] = jnp.concatenate(parts, axis=1).astype(jnp.bfloat16)
        line = bias[h : h + 1, :].astype(jnp.float32)
        lines = [line[:, first : first + PAIR] for first in range(0, length, PAIR)]
        lines += [jnp.zeros((BIAS_ROWS - len(lines), PAIR), jnp.float32)]
        own_ref[h, length : length + BIAS_ROWS, :] = jnp.concatenate(lines, axis=0).astype(
            jnp.bfloat16
        )


def slots_of(n, capacity, routes):
    tokens = routes.shape[1]
    expert = lax.broadcasted_iota(jnp.int32, (n, tokens), 0)
    hits = [(expert == routes[k : k + 1, :]).astype(jnp.float32) for k in range(TOP)]
    earlier = lax.broadcasted_iota(jnp.int32, (tokens, tokens), 0) < lax.broadcasted_iota(
        jnp.int32, (tokens, tokens), 1
    )
    before = jnp.dot(
        sum(hits).astype(jnp.bfloat16),
        earlier.astype(jnp.float32).astype(jnp.bfloat16),
        preferred_element_type=jnp.float32,
    )
    start = before + (expert * capacity).astype(jnp.float32)
    return [jnp.sum(hit * start, axis=0, keepdims=True).astype(jnp.int32) for hit in hits]


def greet_all(n, groups, me, my_t):
    barrier = pltpu.get_barrier_semaphore()

    def greet(device):
        pl.semaphore_signal(barrier, inc=1, device_id=device, device_id_type=MESH)

    def greet_sp(r, carry):
        greet({"sp": lax.rem(me + r, n)})
        return carry

    lax.fori_loop(1, n, greet_sp, 0)
    for k in range(1, groups):
        greet({"tp": lax.rem(my_t + k, groups)})


def layer(
    queries, keys, values, bias, routes, route_weights, residual, out_weight, gain, gate, up, down
):
    n, groups = lax.axis_size("sp"), lax.axis_size("tp")
    chips = groups // 2
    length, width = queries.shape
    heads = bias.shape[0]
    tokens, width_model = residual.shape
    capacity = max(2, 5 * tokens * TOP // (4 * n))
    units = gate.shape[1]
    apart = max(1, chips - 1) * n
    vmem = pl.BlockSpec(memory_space=pltpu.VMEM)
    anywhere = pl.BlockSpec(memory_space=pl.ANY)
    kind = queries.dtype
    return pl.pallas_call(
        functools.partial(layer_kernel, n, groups, length, heads),
        out_shape=jax.ShapeDtypeStruct((tokens, width_model), kind),
        in_specs=[vmem] * 9 + [anywhere] * 3,
        out_specs=vmem,
        scratch_shapes=[
            pltpu.VMEM((heads, length, PAIR), kind),
            pltpu.VMEM((heads, length + BIAS_ROWS, PAIR), kind),
            pltpu.VMEM((n * capacity, tokens), kind),
            pltpu.VMEM((n, capacity, width_model), kind),
            pltpu.VMEM((tokens, width_model), kind),
            pltpu.VMEM(((n + 1) * heads, length + BIAS_ROWS, PAIR), kind),
            pltpu.VMEM((heads, length, PAIR), jnp.float32),
            pltpu.VMEM((heads, length, PAIR), jnp.float32),
            pltpu.VMEM((BLOCK, BLOCK), kind),
            pltpu.VMEM((length, width), kind),
            pltpu.VMEM((groups, tokens, width), kind),
            pltpu.VMEM((n, capacity, width_model), kind),
            pltpu.VMEM((groups * n, capacity, width_model), kind),
            pltpu.VMEM((groups * n, capacity, width_model), kind),
            pltpu.VMEM((groups * capacity, width_model), kind),
            pltpu.VMEM((groups * capacity, units), kind),
            pltpu.VMEM((width_model, units), kind),
            pltpu.VMEM((width_model, units), kind),
            pltpu.VMEM((units, width_model), kind),
            pltpu.VMEM((chips * n, capacity, width_model), kind),
            pltpu.VMEM((apart, capacity, width_model), kind),
            pltpu.VMEM((n, capacity, width_model), kind),
            pltpu.SemaphoreType.DMA(((n + 2) * heads,)),
            pltpu.SemaphoreType.DMA(((n + 2) * heads,)),
            pltpu.SemaphoreType.DMA(((n + 2) * heads,)),
            pltpu.SemaphoreType.DMA((groups,)),
            pltpu.SemaphoreType.DMA((groups,)),
            pltpu.SemaphoreType.DMA((3,)),
            pltpu.SemaphoreType.DMA((n,)),
            pltpu.SemaphoreType.DMA((apart,)),
            pltpu.SemaphoreType.DMA((groups * n,)),
            pltpu.SemaphoreType.DMA((groups * n,)),
            pltpu.SemaphoreType.DMA((chips * n,)),
            pltpu.SemaphoreType.DMA((chips * n,)),
            pltpu.SemaphoreType.DMA((apart,)),
            pltpu.SemaphoreType.DMA((apart,)),
            pltpu.SemaphoreType.DMA((n,)),
            pltpu.SemaphoreType.DMA((n,)),
        ],
        compiler_params=pltpu.CompilerParams(
            collective_id=0, has_side_effects=True, vmem_limit_bytes=62 * 1024 * 1024
        ),
        name="layer",
    )(
        queries, keys, values, bias, routes, route_weights, residual, out_weight, gain,
        gate, up, down,
    )


def shards(
    queries,
    keys,
    values,
    key_bias,
    residual,
    out_weight,
    norm_gain,
    routes,
    route_weights,
    gate_weight,
    up_weight,
    down_weight,
):
    return layer(
        queries, keys, values, jnp.transpose(key_bias), jnp.transpose(routes),
        jnp.transpose(route_weights), residual, out_weight, norm_gain[None, :],
        gate_weight[0], up_weight[0], down_weight[0],
    )


def solution(mesh):
    return jax.shard_map(
        shards,
        mesh=mesh,
        in_specs=(
            P("sp", "tp"),
            P("sp", "tp"),
            P("sp", "tp"),
            P("sp", "tp"),
            P(("sp", "tp"), None),
            P(),
            P(),
            P(("sp", "tp"), None),
            P(("sp", "tp"), None),
            P("sp", None, "tp"),
            P("sp", None, "tp"),
            P("sp", "tp", None),
        ),
        out_specs=P(("sp", "tp"), None),
        check_vma=False,
    )
```

```python
import functools

import jax
import jax.numpy as jnp
from jax import lax
from jax.experimental import pallas as pl
from jax.experimental.pallas import tpu as pltpu
from jax.sharding import PartitionSpec as P

HEAD_DIM = 64
TOP = 2
SPAN = 512
BLOCK = 256
QUERY_ROWS = 256
BIAS_ROWS = 16
PAIR = 2 * HEAD_DIM
WIDE = 512
UNITS = 1024
FEATURES = 2048
MESH = pl.DeviceIdType.MESH


epsilon = 1e-06


def layer_kernel(
    n, groups, length, heads,
    queries, keys, values, bias, routes, route_weights, residual_hbm, out_hbm, gain,
    gate_hbm, up_hbm, down_hbm, out,
    residual, out_weight, q_ref, own_ref, place, back, mixed, held, total, after, tri, attended, heads_in, outgoing, rows, partial, block, hidden,
    gate, up_w, down, pair, other, done,
    up_sem, side_sem, recv_sem, share_send, share_recv, weight_sem, sp_sem, chip_sem, core_sem,
    row_sem, pair_send, pair_recv, chip_send, chip_recv, back_send, back_recv,
):
    me, my_t = lax.axis_index("sp"), lax.axis_index("tp")
    odd = lax.rem(me, 2)
    level = me // 2
    partner = me + 1 - 2 * odd
    has_up = me + 2 < n
    core = lax.rem(my_t, 2)
    mate = my_t + 1 - 2 * core
    chips = groups // 2
    alike = [lax.rem(my_t + 2 * k, groups) for k in range(1, chips)]
    loads = [
        pltpu.make_async_copy(gate_hbm, gate, weight_sem.at[0]),
        pltpu.make_async_copy(up_hbm, up_w, weight_sem.at[1]),
        pltpu.make_async_copy(down_hbm, down, weight_sem.at[2]),
    ]
    first_loads = [
        pltpu.make_async_copy(residual_hbm, residual, weight_sem.at[3]),
        pltpu.make_async_copy(out_hbm, out_weight, weight_sem.at[4]),
    ]
    for load in first_loads:
        load.start()
    greet_all(n, groups, me, my_t)
    build_heads(length, heads, queries, keys, values, bias, q_ref, own_ref)
    capacity = outgoing.shape[1]
    slots = slots_of(n, capacity, routes)
    for first in range(0, n * capacity, 64):
        slot = first + lax.broadcasted_iota(jnp.int32, (64, routes.shape[1]), 0)
        hit = jnp.zeros(slot.shape, jnp.float32)
        for row in slots:
            hit = hit + (slot == row).astype(jnp.float32)
        place[first : first + 64, :] = hit.astype(jnp.bfloat16)
    total[...] = jnp.zeros_like(total)
    after[...] = jnp.zeros_like(after)
    tri_row = lax.broadcasted_iota(jnp.int32, (BLOCK, BLOCK), 0)
    tri_col = lax.broadcasted_iota(jnp.int32, (BLOCK, BLOCK), 1)
    tri[...] = (tri_row > tri_col).astype(jnp.float32).astype(jnp.bfloat16)
    pl.semaphore_wait(pltpu.get_barrier_semaphore(), n - 1 + groups - 1)

    def up(d, h, source):
        return pltpu.make_async_remote_copy(
            src_ref=source,
            dst_ref=held.at[(d + 2) * heads + h],
            send_sem=up_sem.at[d * heads + h],
            recv_sem=recv_sem.at[(d + 2) * heads + h],
            device_id={"sp": me + 2},
            device_id_type=MESH,
        )

    def side(d, h, slot, source):
        return pltpu.make_async_remote_copy(
            src_ref=source,
            dst_ref=held.at[slot * heads + h],
            send_sem=side_sem.at[d * heads + h],
            recv_sem=recv_sem.at[slot * heads + h],
            device_id={"sp": partner},
            device_id_type=MESH,
        )

    def send(d, h, source):
        pl.when(has_up)(lambda: up(d, h, source).start())
        pl.when(odd == 0)(lambda: side(d, h, d + 1, source).start())
        pl.when((odd == 1) & (d >= 2))(lambda: side(d, h, d - 1, source).start())

    def sent(d, h, source):
        pl.when(has_up)(lambda: up(d, h, source).wait_send())
        pl.when(odd == 0)(lambda: side(d, h, d + 1, source).wait_send())
        pl.when((odd == 1) & (d >= 2))(lambda: side(d, h, d - 1, source).wait_send())

    def arrived(d, h):
        pltpu.make_async_remote_copy(
            src_ref=held.at[d * heads + h],
            dst_ref=held.at[d * heads + h],
            send_sem=up_sem.at[d * heads + h],
            recv_sem=recv_sem.at[d * heads + h],
            device_id={"sp": partner},
            device_id_type=MESH,
        ).wait_recv()

    per_block = BLOCK // PAIR

    def attend_rows(sources, q0, todo, masked):
        rows = pl.ds(q0, QUERY_ROWS)
        units = [(h, block) for block in todo for h in range(heads)]
        rest, soft, beyond = {}, {}, {}
        earlier = None
        if masked is not None:
            earlier = lax.broadcasted_iota(
                jnp.int32, (QUERY_ROWS, BLOCK), 1
            ) < lax.broadcasted_iota(jnp.int32, (QUERY_ROWS, BLOCK), 0)
        for h, block in units:
            b0 = block * BLOCK
            bias = sources[h][length : length + BIAS_ROWS, :].astype(jnp.float32)
            bias_row = jnp.concatenate(
                [
                    bias[block * per_block + i : block * per_block + i + 1]
                    for i in range(per_block)
                ],
                axis=1,
            )
            scores = lax.dot_general(
                q_ref[h, rows, :],
                sources[h][b0 : b0 + BLOCK, :],
                (((1,), (1,)), ((), ())),
                preferred_element_type=jnp.float32,
            )
            scores = scores + bias_row
            value = jnp.maximum(scores, 0.0) + jnp.log(1.0 + jnp.exp(-jnp.abs(scores)))
            rest[h, block] = scores - value
            if block == masked:
                value = jnp.where(earlier, value, 0.0)
            soft[h, block] = value
            beyond[h, block] = jnp.dot(
                value.astype(jnp.bfloat16), tri[...], preferred_element_type=jnp.float32
            )
        for h in range(heads):
            later = after[h, rows, :]
            gathered = total[h, rows, :]
            for block in todo:
                b0 = block * BLOCK
                past = beyond[h, block]
                piece = jnp.exp(rest[h, block] - past - jnp.concatenate([later] * per_block, axis=1))
                if block == masked:
                    piece = jnp.where(earlier, piece, 0.0)
                gathered = gathered + jnp.dot(
                    piece.astype(jnp.bfloat16),
                    sources[h][b0 : b0 + BLOCK, :],
                    preferred_element_type=jnp.float32,
                )
                later = later + (past[:, :1] + soft[h, block][:, :1])
            total[h, rows, :] = gathered
            after[h, rows, :] = later

    blocks = length // BLOCK

    def compute_own():
        sources = [own_ref.at[h] for h in range(heads)]
        for c in range(blocks):
            attend_rows(sources, c * BLOCK, list(reversed(range(c + 1))), c)

    def compute(d):
        sources = [held.at[d * heads + h] for h in range(heads)]

        def chunk(c, carry):
            q0 = pl.multiple_of(c * QUERY_ROWS, QUERY_ROWS)
            attend_rows(sources, q0, list(reversed(range(blocks))), None)
            return carry

        lax.fori_loop(0, length // QUERY_ROWS, chunk, 0)

    for h in range(heads):
        send(0, h, own_ref.at[h])
    compute_own()
    for load in loads:
        load.start()

    def step(k, carry):
        @pl.when(k <= level)
        def _():
            for h in range(heads):
                arrived(2 * k, h)
                send(2 * k, h, held.at[2 * k * heads + h])

        first = 2 * k - 3 + 2 * odd

        @pl.when(first >= 1)
        def _():
            for h in range(heads):
                arrived(first, h)

        def one(d, inner):
            compute(d)
            return inner

        lax.fori_loop(jnp.maximum(first, 1), jnp.minimum(first + 1, me) + 1, one, 0)
        return carry

    lax.fori_loop(1, level + 2, step, 0)
    lane = lax.broadcasted_iota(jnp.int32, (length, PAIR), 1)
    for h in range(0, heads, 2):
        joined = total[h]
        if h + 1 < heads:
            joined = jnp.where(lane >= HEAD_DIM, total[h + 1], joined)
        columns = min(PAIR, (heads - h) * HEAD_DIM)
        attended[:, h * HEAD_DIM : h * HEAD_DIM + columns] = joined[:, :columns].astype(jnp.bfloat16)


    tokens, width_model = residual.shape

    def share(k):
        target = lax.rem(my_t + k, groups)
        return pltpu.make_async_remote_copy(
            src_ref=attended.at[pl.ds(pl.multiple_of(target * tokens, tokens), tokens)],
            dst_ref=heads_in.at[my_t],
            send_sem=share_send.at[k],
            recv_sem=share_recv.at[my_t],
            device_id={"tp": target},
            device_id_type=MESH,
        )

    def shared(t):
        pltpu.make_async_remote_copy(
            src_ref=heads_in.at[t],
            dst_ref=heads_in.at[t],
            send_sem=share_send.at[0],
            recv_sem=share_recv.at[t],
            device_id={"tp": mate},
            device_id_type=MESH,
        ).wait_recv()

    for k in range(1, groups):
        share(k).start()
    heads_in[my_t] = attended[pl.ds(pl.multiple_of(my_t * tokens, tokens), tokens)]
    for k in range(1, groups):
        shared(lax.rem(my_t + k, groups))
    for load in first_loads:
        load.wait()
    token_heads = jnp.concatenate([heads_in[t] for t in range(groups)], axis=1)
    squares = jnp.zeros((tokens, 1), jnp.float32)
    wide = min(WIDE, width_model)
    for first in range(0, width_model, wide):
        columns = slice(first, first + wide)
        projected = jnp.dot(token_heads, out_weight[:, columns], preferred_element_type=jnp.float32)
        piece = (residual[:, columns].astype(jnp.float32) + projected).astype(jnp.bfloat16)
        mixed[:, columns] = piece
        piece = piece.astype(jnp.float32)
        squares = squares + jnp.sum(piece * piece, axis=1, keepdims=True)
    scale = lax.rsqrt(squares / width_model + epsilon)
    for first in range(0, width_model, wide):
        columns = slice(first, first + wide)
        piece = mixed[:, columns].astype(jnp.float32) * scale * gain[:, columns]
        placed = jnp.dot(place[...], piece.astype(jnp.bfloat16), preferred_element_type=jnp.float32)
        for e in range(n):
            outgoing[e, :, columns] = placed[e * capacity : (e + 1) * capacity].astype(jnp.bfloat16)

    def copy(source, t, s, send_sem, device):
        return pltpu.make_async_remote_copy(
            src_ref=source,
            dst_ref=rows.at[t * n + s],
            send_sem=send_sem,
            recv_sem=row_sem.at[t * n + s],
            device_id=device,
            device_id_type=MESH,
        )

    def to_expert(r):
        target = lax.rem(me + r, n)
        return copy(outgoing.at[target], my_t, me, sp_sem.at[r], {"sp": target})

    def to_chip(k, s, source):
        return copy(source, my_t, s, chip_sem.at[k * n + s], {"tp": alike[k]})

    def to_mate(t, s, source):
        return copy(source, t, s, core_sem.at[t * n + s], {"tp": mate})

    def row_arrived(t, s):
        copy(rows.at[t * n + s], t, s, core_sem.at[t * n + s], {"tp": mate}).wait_recv()

    def spread(s, source):
        for k in range(chips - 1):
            to_chip(k, s, source).start()
        to_mate(my_t, s, source).start()

    def issue(r, carry):
        to_expert(r).start()
        return carry

    spread(me, outgoing.at[me])
    lax.fori_loop(1, n, issue, 0)
    rows[my_t * n + me] = outgoing[me]
    for load in loads:
        load.wait()

    orders = take_orders(n)
    sources = [
        sum((me == i).astype(jnp.int32) * orders[i][j] for i in range(n)) for j in range(n)
    ]

    def source_of(j):
        return sum((j == i).astype(jnp.int32) * sources[i] for i in range(n))

    def take(j):
        s = source_of(j)

        @pl.when(s != me)
        def _():
            row_arrived(my_t, s)
            spread(s, rows.at[my_t * n + s])

    def relay(j):
        s = source_of(j)
        for t in alike:
            row_arrived(t, s)
            to_mate(t, s, rows.at[t * n + s]).start()

    def expert(j):
        s = source_of(j)
        row_arrived(mate, s)
        for t in alike:
            row_arrived(t + 1 - 2 * lax.rem(t, 2), s)
        block[...] = jnp.concatenate([rows[t * n + s] for t in range(groups)], axis=0)
        unit_step = min(UNITS, gate.shape[1])

        def units(f, carry):
            columns = pl.ds(pl.multiple_of(f * unit_step, unit_step), unit_step)
            gate_act = jnp.dot(block[...], gate[:, columns], preferred_element_type=jnp.float32)
            up_act = jnp.dot(block[...], up_w[:, columns], preferred_element_type=jnp.float32)
            silu = gate_act / (1.0 + jnp.exp(-gate_act))
            hidden[:, columns] = (silu * up_act).astype(jnp.bfloat16)
            return carry

        lax.fori_loop(0, gate.shape[1] // unit_step, units, 0)
        step = min(FEATURES, width_model)

        def features(f, carry):
            columns = pl.ds(pl.multiple_of(f * step, step), step)
            value = jnp.dot(hidden[...], down[:, columns], preferred_element_type=jnp.float32)
            for t in range(groups):
                piece = value[t * capacity : (t + 1) * capacity]
                partial[t * n + s, :, columns] = piece.astype(jnp.bfloat16)
            return carry

        lax.fori_loop(0, width_model // step, features, 0)
        for chip in range(chips):
            pair_copy(chip, j).start()

    def pair_copy(chip, j):
        return pltpu.make_async_remote_copy(
            src_ref=partial.at[(2 * chip + 1 - core) * n + source_of(j)],
            dst_ref=pair.at[chip * n + j],
            send_sem=pair_send.at[chip * n + j],
            recv_sem=pair_recv.at[chip * n + j],
            device_id={"tp": mate},
            device_id_type=MESH,
        )

    def chip_copy(k, j):
        return pltpu.make_async_remote_copy(
            src_ref=pair.at[(alike[k] // 2) * n + j],
            dst_ref=other.at[k * n + j],
            send_sem=chip_send.at[k * n + j],
            recv_sem=chip_recv.at[k * n + j],
            device_id={"tp": alike[k]},
            device_id_type=MESH,
        )

    def back_copy(j):
        return pltpu.make_async_remote_copy(
            src_ref=done.at[j],
            dst_ref=back.at[me],
            send_sem=back_send.at[j],
            recv_sem=back_recv.at[me],
            device_id={"sp": source_of(j)},
            device_id_type=MESH,
        )

    def sum_pairs(j):
        for chip in range(chips):
            pair_copy(chip, j).wait_recv()
        for k in range(chips - 1):
            chip = alike[k] // 2
            pair[chip * n + j] = (
                partial[alike[k] * n + source_of(j)].astype(jnp.float32)
                + pair[chip * n + j].astype(jnp.float32)
            ).astype(jnp.bfloat16)
        for k in range(chips - 1):
            chip_copy(k, j).start()

    def give_back(j):
        s = source_of(j)
        value = partial[my_t * n + s].astype(jnp.float32) + pair[(my_t // 2) * n + j].astype(
            jnp.float32
        )
        for k in range(chips - 1):
            chip_copy(k, j).wait_recv()
            value = value + other[k * n + j].astype(jnp.float32)
        value = value.astype(jnp.bfloat16)

        @pl.when(s == me)
        def _():
            back[me] = value

        @pl.when(s != me)
        def _():
            done[j] = value
            back_copy(j).start()

    def flow(j, carry):
        pl.when((j >= 4) & (j < n + 4))(lambda: give_back(j - 4))
        pl.when((j >= 3) & (j < n + 3))(lambda: sum_pairs(j - 3))
        pl.when((j >= 2) & (j < n + 2))(lambda: expert(j - 2))
        pl.when(j < n)(lambda: take(j))
        pl.when((j >= 1) & (j < n + 1))(lambda: relay(j - 1))
        return carry

    lax.fori_loop(0, n + 4, flow, 0)

    for h in range(heads):
        sent(0, h, own_ref.at[h])

    def drain(k, carry):
        for h in range(heads):
            sent(2 * k, h, held.at[2 * k * heads + h])
        return carry

    lax.fori_loop(1, level + 1, drain, 0)

    for k in range(1, groups):
        share(k).wait_send()

    def finish(j, carry):
        s = source_of(j)
        pl.when(j >= 1)(lambda: to_expert(j).wait_send())
        for k in range(chips - 1):
            to_chip(k, s, outgoing.at[me]).wait_send()
            to_mate(alike[k], s, outgoing.at[me]).wait_send()
            chip_copy(k, j).wait_send()
        to_mate(my_t, s, outgoing.at[me]).wait_send()
        for chip in range(chips):
            pair_copy(chip, j).wait_send()

        @pl.when(s != me)
        def _():
            back_copy(j).wait_send()
            pltpu.make_async_remote_copy(
                src_ref=done.at[j],
                dst_ref=back.at[s],
                send_sem=back_send.at[j],
                recv_sem=back_recv.at[s],
                device_id={"sp": s},
                device_id_type=MESH,
            ).wait_recv()

        return carry

    lax.fori_loop(0, n, finish, 0)
    extra = [row.astype(jnp.float32) for row in slots]
    extra += [route_weights[k : k + 1, :] for k in range(TOP)]
    extra += [jnp.zeros((8 - len(extra), tokens), jnp.float32)]
    across = jnp.transpose(jnp.concatenate(extra, axis=0))
    slot = lax.broadcasted_iota(jnp.int32, (tokens, n * capacity), 1)
    select = [
        (slot == across[:, k : k + 1].astype(jnp.int32)).astype(jnp.float32).astype(jnp.bfloat16)
        for k in range(TOP)
    ]
    for first in range(0, width_model, wide):
        columns = slice(first, first + wide)
        returned = jnp.concatenate([back[e, :, columns] for e in range(n)], axis=0)
        value = mixed[:, columns].astype(jnp.float32)
        routed = jnp.zeros((tokens, wide), jnp.float32)
        for k in range(TOP):
            picked = jnp.dot(select[k], returned, preferred_element_type=jnp.float32)
            routed = routed + picked * across[:, TOP + k : TOP + k + 1]
        out[:, columns] = (value + routed).astype(out.dtype)


def build_heads(length, heads, queries, keys, values, bias, q_ref, own_ref):
    for h in range(heads):
        columns = slice(h * HEAD_DIM, (h + 1) * HEAD_DIM)
        order = 1 if h % 2 == 0 else -1
        for first in range(0, length, 256):
            rows = slice(first, first + 256)
            query = queries[rows, columns].astype(jnp.float32) * HEAD_DIM ** (-0.5)
            parts = [jnp.zeros_like(query), query][::order]
            q_ref[h, rows, :] = jnp.concatenate(parts, axis=1).astype(jnp.bfloat16)
            parts = [values[rows, columns], keys[rows, columns]][::order]
            parts = [part.astype(jnp.float32) for part in parts]
            own_ref[h, rows, :] = jnp.concatenate(parts, axis=1).astype(jnp.bfloat16)
        line = bias[h : h + 1, :].astype(jnp.float32)
        lines = [line[:, first : first + PAIR] for first in range(0, length, PAIR)]
        lines += [jnp.zeros((BIAS_ROWS - len(lines), PAIR), jnp.float32)]
        own_ref[h, length : length + BIAS_ROWS, :] = jnp.concatenate(lines, axis=0).astype(
            jnp.bfloat16
        )


def slots_of(n, capacity, routes):
    tokens = routes.shape[1]
    expert = lax.broadcasted_iota(jnp.int32, (n, tokens), 0)
    hits = [(expert == routes[k : k + 1, :]).astype(jnp.float32) for k in range(TOP)]
    earlier = lax.broadcasted_iota(jnp.int32, (tokens, tokens), 0) < lax.broadcasted_iota(
        jnp.int32, (tokens, tokens), 1
    )
    before = jnp.dot(
        sum(hits).astype(jnp.bfloat16),
        earlier.astype(jnp.float32).astype(jnp.bfloat16),
        preferred_element_type=jnp.float32,
    )
    start = before + (expert * capacity).astype(jnp.float32)
    return [jnp.sum(hit * start, axis=0, keepdims=True).astype(jnp.int32) for hit in hits]


def take_orders(n):
    orders = [[(me + n - j) % n for j in range(n)] for me in range(n)]
    if n == 8:
        for me, order in [(6, [6, 7, 0, 1, 2, 3, 4, 5]), (7, [7, 6, 1, 0, 3, 2, 5, 4]), (0, [0, 1, 2, 3, 7, 6, 5, 4]), (1, [1, 0, 3, 2, 6, 7, 4, 5]), (4, [4, 5, 3, 2, 1, 0, 7, 6]), (5, [5, 4, 2, 3, 0, 1, 6, 7])]:
            orders[me] = order
    return orders


def greet_all(n, groups, me, my_t):
    barrier = pltpu.get_barrier_semaphore()

    def greet(device):
        pl.semaphore_signal(barrier, inc=1, device_id=device, device_id_type=MESH)

    def greet_sp(r, carry):
        greet({"sp": lax.rem(me + r, n)})
        return carry

    lax.fori_loop(1, n, greet_sp, 0)
    for k in range(1, groups):
        greet({"tp": lax.rem(my_t + k, groups)})


def layer(
    queries, keys, values, bias, routes, route_weights, residual, out_weight, gain, gate, up, down
):
    n, groups = lax.axis_size("sp"), lax.axis_size("tp")
    chips = groups // 2
    length, width = queries.shape
    heads = bias.shape[0]
    tokens, width_model = residual.shape
    capacity = max(2, 5 * tokens * TOP // (4 * n))
    units = gate.shape[1]
    apart = max(1, chips - 1) * n
    vmem = pl.BlockSpec(memory_space=pltpu.VMEM)
    anywhere = pl.BlockSpec(memory_space=pl.ANY)
    kind = queries.dtype
    return pl.pallas_call(
        functools.partial(layer_kernel, n, groups, length, heads),
        out_shape=jax.ShapeDtypeStruct((tokens, width_model), kind),
        in_specs=[vmem] * 6 + [anywhere] * 2 + [vmem] + [anywhere] * 3,
        out_specs=vmem,
        scratch_shapes=[
            pltpu.VMEM((tokens, width_model), kind),
            pltpu.VMEM(out_weight.shape, kind),
            pltpu.VMEM((heads, length, PAIR), kind),
            pltpu.VMEM((heads, length + BIAS_ROWS, PAIR), kind),
            pltpu.VMEM((n * capacity, tokens), kind),
            pltpu.VMEM((n, capacity, width_model), kind),
            pltpu.VMEM((tokens, width_model), kind),
            pltpu.VMEM(((n + 1) * heads, length + BIAS_ROWS, PAIR), kind),
            pltpu.VMEM((heads, length, PAIR), jnp.float32),
            pltpu.VMEM((heads, length, PAIR), jnp.float32),
            pltpu.VMEM((BLOCK, BLOCK), kind),
            pltpu.VMEM((length, width), kind),
            pltpu.VMEM((groups, tokens, width), kind),
            pltpu.VMEM((n, capacity, width_model), kind),
            pltpu.VMEM((groups * n, capacity, width_model), kind),
            pltpu.VMEM((groups * n, capacity, width_model), kind),
            pltpu.VMEM((groups * capacity, width_model), kind),
            pltpu.VMEM((groups * capacity, units), kind),
            pltpu.VMEM((width_model, units), kind),
            pltpu.VMEM((width_model, units), kind),
            pltpu.VMEM((units, width_model), kind),
            pltpu.VMEM((chips * n, capacity, width_model), kind),
            pltpu.VMEM((apart, capacity, width_model), kind),
            pltpu.VMEM((n, capacity, width_model), kind),
            pltpu.SemaphoreType.DMA(((n + 2) * heads,)),
            pltpu.SemaphoreType.DMA(((n + 2) * heads,)),
            pltpu.SemaphoreType.DMA(((n + 2) * heads,)),
            pltpu.SemaphoreType.DMA((groups,)),
            pltpu.SemaphoreType.DMA((groups,)),
            pltpu.SemaphoreType.DMA((5,)),
            pltpu.SemaphoreType.DMA((n,)),
            pltpu.SemaphoreType.DMA((apart,)),
            pltpu.SemaphoreType.DMA((groups * n,)),
            pltpu.SemaphoreType.DMA((groups * n,)),
            pltpu.SemaphoreType.DMA((chips * n,)),
            pltpu.SemaphoreType.DMA((chips * n,)),
            pltpu.SemaphoreType.DMA((apart,)),
            pltpu.SemaphoreType.DMA((apart,)),
            pltpu.SemaphoreType.DMA((n,)),
            pltpu.SemaphoreType.DMA((n,)),
        ],
        compiler_params=pltpu.CompilerParams(
            collective_id=0, has_side_effects=True, vmem_limit_bytes=62 * 1024 * 1024
        ),
        name="layer",
    )(
        queries, keys, values, bias, routes, route_weights, residual, out_weight, gain,
        gate, up, down,
    )


def shards(
    queries,
    keys,
    values,
    key_bias,
    residual,
    out_weight,
    norm_gain,
    routes,
    route_weights,
    gate_weight,
    up_weight,
    down_weight,
):
    return layer(
        queries, keys, values, jnp.transpose(key_bias), jnp.transpose(routes),
        jnp.transpose(route_weights), residual, out_weight, norm_gain[None, :],
        gate_weight[0], up_weight[0], down_weight[0],
    )


def solution(mesh):
    return jax.shard_map(
        shards,
        mesh=mesh,
        in_specs=(
            P("sp", "tp"),
            P("sp", "tp"),
            P("sp", "tp"),
            P("sp", "tp"),
            P(("sp", "tp"), None),
            P(),
            P(),
            P(("sp", "tp"), None),
            P(("sp", "tp"), None),
            P("sp", None, "tp"),
            P("sp", None, "tp"),
            P("sp", "tp", None),
        ),
        out_specs=P(("sp", "tp"), None),
        check_vma=False,
    )
```

```python
import functools

import jax
import jax.numpy as jnp
from jax import lax
from jax.experimental import pallas as pl
from jax.experimental.pallas import tpu as pltpu
from jax.sharding import PartitionSpec as P

HEAD_DIM = 64
TOP = 2
SPAN = 512
BLOCK = 256
QUERY_ROWS = 256
BIAS_ROWS = 16
PAIR = 2 * HEAD_DIM
WIDE = 1024
UNITS = 1024
FEATURES = 2048
MESH = pl.DeviceIdType.MESH


epsilon = 1e-06


def layer_kernel(
    n, groups, length, heads,
    queries, keys, values, bias, routes, route_weights, residual_hbm, out_hbm, gain,
    gate_hbm, up_hbm, down_hbm, out,
    residual, out_weight, q_ref, own_ref, place, back, mixed, held, total, after, tri, attended, heads_in, outgoing, rows, partial, block, hidden,
    gate, up_w, down, pair, other, done,
    up_sem, side_sem, recv_sem, share_send, share_recv, weight_sem, sp_sem, chip_sem, core_sem,
    row_sem, pair_send, pair_recv, chip_send, chip_recv, back_send, back_recv,
):
    me, my_t = lax.axis_index("sp"), lax.axis_index("tp")
    odd = lax.rem(me, 2)
    level = me // 2
    partner = me + 1 - 2 * odd
    has_up = me + 2 < n
    core = lax.rem(my_t, 2)
    mate = my_t + 1 - 2 * core
    chips = groups // 2
    alike = [lax.rem(my_t + 2 * k, groups) for k in range(1, chips)]
    loads = [
        pltpu.make_async_copy(gate_hbm, gate, weight_sem.at[0]),
        pltpu.make_async_copy(up_hbm, up_w, weight_sem.at[1]),
        pltpu.make_async_copy(down_hbm, down, weight_sem.at[2]),
    ]
    first_loads = [
        pltpu.make_async_copy(residual_hbm, residual, weight_sem.at[3]),
        pltpu.make_async_copy(out_hbm, out_weight, weight_sem.at[4]),
    ]
    for load in first_loads:
        load.start()
    greet_all(n, groups, me, my_t)
    build_heads(length, heads, queries, keys, values, bias, q_ref, own_ref)
    capacity = outgoing.shape[1]
    slots = slots_of(n, capacity, routes)
    for first in range(0, n * capacity, 64):
        slot = first + lax.broadcasted_iota(jnp.int32, (64, routes.shape[1]), 0)
        hit = jnp.zeros(slot.shape, jnp.float32)
        for row in slots:
            hit = hit + (slot == row).astype(jnp.float32)
        place[first : first + 64, :] = hit.astype(jnp.bfloat16)
    total[...] = jnp.zeros_like(total)
    after[...] = jnp.zeros_like(after)
    tri_row = lax.broadcasted_iota(jnp.int32, (BLOCK, BLOCK), 0)
    tri_col = lax.broadcasted_iota(jnp.int32, (BLOCK, BLOCK), 1)
    tri[...] = (tri_row > tri_col).astype(jnp.float32).astype(jnp.bfloat16)
    pl.semaphore_wait(pltpu.get_barrier_semaphore(), n - 1 + groups - 1)

    def up(d, h, source):
        return pltpu.make_async_remote_copy(
            src_ref=source,
            dst_ref=held.at[(d + 2) * heads + h],
            send_sem=up_sem.at[d * heads + h],
            recv_sem=recv_sem.at[(d + 2) * heads + h],
            device_id={"sp": me + 2},
            device_id_type=MESH,
        )

    def side(d, h, slot, source):
        return pltpu.make_async_remote_copy(
            src_ref=source,
            dst_ref=held.at[slot * heads + h],
            send_sem=side_sem.at[d * heads + h],
            recv_sem=recv_sem.at[slot * heads + h],
            device_id={"sp": partner},
            device_id_type=MESH,
        )

    def send(d, h, source):
        pl.when(has_up)(lambda: up(d, h, source).start())
        pl.when(odd == 0)(lambda: side(d, h, d + 1, source).start())
        pl.when((odd == 1) & (d >= 2))(lambda: side(d, h, d - 1, source).start())

    def sent(d, h, source):
        pl.when(has_up)(lambda: up(d, h, source).wait_send())
        pl.when(odd == 0)(lambda: side(d, h, d + 1, source).wait_send())
        pl.when((odd == 1) & (d >= 2))(lambda: side(d, h, d - 1, source).wait_send())

    def arrived(d, h):
        pltpu.make_async_remote_copy(
            src_ref=held.at[d * heads + h],
            dst_ref=held.at[d * heads + h],
            send_sem=up_sem.at[d * heads + h],
            recv_sem=recv_sem.at[d * heads + h],
            device_id={"sp": partner},
            device_id_type=MESH,
        ).wait_recv()

    per_block = BLOCK // PAIR

    def attend_rows(sources, q0, todo, masked):
        rows = pl.ds(q0, QUERY_ROWS)
        units = [(h, block) for block in todo for h in range(heads)]
        rest, soft, beyond = {}, {}, {}
        earlier = None
        if masked is not None:
            earlier = lax.broadcasted_iota(
                jnp.int32, (QUERY_ROWS, BLOCK), 1
            ) < lax.broadcasted_iota(jnp.int32, (QUERY_ROWS, BLOCK), 0)
        for h, block in units:
            b0 = block * BLOCK
            bias = sources[h][length : length + BIAS_ROWS, :].astype(jnp.float32)
            bias_row = jnp.concatenate(
                [
                    bias[block * per_block + i : block * per_block + i + 1]
                    for i in range(per_block)
                ],
                axis=1,
            )
            scores = lax.dot_general(
                q_ref[h, rows, :],
                sources[h][b0 : b0 + BLOCK, :],
                (((1,), (1,)), ((), ())),
                preferred_element_type=jnp.float32,
            )
            scores = scores + bias_row
            value = jnp.maximum(scores, 0.0) + jnp.log(1.0 + jnp.exp(-jnp.abs(scores)))
            rest[h, block] = scores - value
            if block == masked:
                value = jnp.where(earlier, value, 0.0)
            soft[h, block] = value
            beyond[h, block] = jnp.dot(
                value.astype(jnp.bfloat16), tri[...], preferred_element_type=jnp.float32
            )
        for h in range(heads):
            later = after[h, rows, :]
            gathered = total[h, rows, :]
            for block in todo:
                b0 = block * BLOCK
                past = beyond[h, block]
                piece = jnp.exp(rest[h, block] - past - jnp.concatenate([later] * per_block, axis=1))
                if block == masked:
                    piece = jnp.where(earlier, piece, 0.0)
                gathered = gathered + jnp.dot(
                    piece.astype(jnp.bfloat16),
                    sources[h][b0 : b0 + BLOCK, :],
                    preferred_element_type=jnp.float32,
                )
                later = later + (past[:, :1] + soft[h, block][:, :1])
            total[h, rows, :] = gathered
            after[h, rows, :] = later

    blocks = length // BLOCK

    def compute_own():
        sources = [own_ref.at[h] for h in range(heads)]
        for c in range(blocks):
            attend_rows(sources, c * BLOCK, list(reversed(range(c + 1))), c)

    def compute(d):
        sources = [held.at[d * heads + h] for h in range(heads)]

        def chunk(c, carry):
            q0 = pl.multiple_of(c * QUERY_ROWS, QUERY_ROWS)
            attend_rows(sources, q0, list(reversed(range(blocks))), None)
            return carry

        lax.fori_loop(0, length // QUERY_ROWS, chunk, 0)

    for h in range(heads):
        send(0, h, own_ref.at[h])
    compute_own()
    for load in loads:
        load.start()

    def step(k, carry):
        @pl.when(k <= level)
        def _():
            for h in range(heads):
                arrived(2 * k, h)
                send(2 * k, h, held.at[2 * k * heads + h])

        first = 2 * k - 3 + 2 * odd

        @pl.when(first >= 1)
        def _():
            for h in range(heads):
                arrived(first, h)

        def one(d, inner):
            compute(d)
            return inner

        lax.fori_loop(jnp.maximum(first, 1), jnp.minimum(first + 1, me) + 1, one, 0)
        return carry

    lax.fori_loop(1, level + 2, step, 0)
    lane = lax.broadcasted_iota(jnp.int32, (length, PAIR), 1)
    for h in range(0, heads, 2):
        joined = total[h]
        if h + 1 < heads:
            joined = jnp.where(lane >= HEAD_DIM, total[h + 1], joined)
        columns = min(PAIR, (heads - h) * HEAD_DIM)
        attended[:, h * HEAD_DIM : h * HEAD_DIM + columns] = joined[:, :columns].astype(jnp.bfloat16)


    tokens, width_model = residual.shape

    def share(k):
        target = lax.rem(my_t + k, groups)
        return pltpu.make_async_remote_copy(
            src_ref=attended.at[pl.ds(pl.multiple_of(target * tokens, tokens), tokens)],
            dst_ref=heads_in.at[my_t],
            send_sem=share_send.at[k],
            recv_sem=share_recv.at[my_t],
            device_id={"tp": target},
            device_id_type=MESH,
        )

    def shared(t):
        pltpu.make_async_remote_copy(
            src_ref=heads_in.at[t],
            dst_ref=heads_in.at[t],
            send_sem=share_send.at[0],
            recv_sem=share_recv.at[t],
            device_id={"tp": mate},
            device_id_type=MESH,
        ).wait_recv()

    for k in range(1, groups):
        share(k).start()
    heads_in[my_t] = attended[pl.ds(pl.multiple_of(my_t * tokens, tokens), tokens)]
    for k in range(1, groups):
        shared(lax.rem(my_t + k, groups))
    for load in first_loads:
        load.wait()
    token_heads = jnp.concatenate([heads_in[t] for t in range(groups)], axis=1)
    squares = jnp.zeros((tokens, 1), jnp.float32)
    wide = min(WIDE, width_model)
    for first in range(0, width_model, wide):
        columns = slice(first, first + wide)
        projected = jnp.dot(token_heads, out_weight[:, columns], preferred_element_type=jnp.float32)
        piece = (residual[:, columns].astype(jnp.float32) + projected).astype(jnp.bfloat16)
        mixed[:, columns] = piece
        piece = piece.astype(jnp.float32)
        squares = squares + jnp.sum(piece * piece, axis=1, keepdims=True)
    scale = lax.rsqrt(squares / width_model + epsilon)
    for first in range(0, width_model, wide):
        columns = slice(first, first + wide)
        piece = mixed[:, columns].astype(jnp.float32) * scale * gain[:, columns]
        placed = jnp.dot(place[...], piece.astype(jnp.bfloat16), preferred_element_type=jnp.float32)
        for e in range(n):
            outgoing[e, :, columns] = placed[e * capacity : (e + 1) * capacity].astype(jnp.bfloat16)

    def copy(source, t, s, send_sem, device):
        return pltpu.make_async_remote_copy(
            src_ref=source,
            dst_ref=rows.at[t * n + s],
            send_sem=send_sem,
            recv_sem=row_sem.at[t * n + s],
            device_id=device,
            device_id_type=MESH,
        )

    def to_expert(r):
        target = lax.rem(me + r, n)
        return copy(outgoing.at[target], my_t, me, sp_sem.at[r], {"sp": target})

    def to_chip(k, s, source):
        return copy(source, my_t, s, chip_sem.at[k * n + s], {"tp": alike[k]})

    def to_mate(t, s, source):
        return copy(source, t, s, core_sem.at[t * n + s], {"tp": mate})

    def row_arrived(t, s):
        copy(rows.at[t * n + s], t, s, core_sem.at[t * n + s], {"tp": mate}).wait_recv()

    def spread(s, source):
        for k in range(chips - 1):
            to_chip(k, s, source).start()
        to_mate(my_t, s, source).start()

    def issue(r, carry):
        to_expert(r).start()
        return carry

    spread(me, outgoing.at[me])
    lax.fori_loop(1, n, issue, 0)
    rows[my_t * n + me] = outgoing[me]
    for load in loads:
        load.wait()

    orders = take_orders(n)
    sources = [
        sum((me == i).astype(jnp.int32) * orders[i][j] for i in range(n)) for j in range(n)
    ]

    def source_of(j):
        return sum((j == i).astype(jnp.int32) * sources[i] for i in range(n))

    def take(j):
        s = source_of(j)

        @pl.when(s != me)
        def _():
            row_arrived(my_t, s)
            spread(s, rows.at[my_t * n + s])

    def relay(j):
        s = source_of(j)
        for t in alike:
            row_arrived(t, s)
            to_mate(t, s, rows.at[t * n + s]).start()

    def expert(j):
        s = source_of(j)
        row_arrived(mate, s)
        for t in alike:
            row_arrived(t + 1 - 2 * lax.rem(t, 2), s)
        block[...] = jnp.concatenate([rows[t * n + s] for t in range(groups)], axis=0)
        unit_step = min(UNITS, gate.shape[1])

        def units(f, carry):
            columns = pl.ds(pl.multiple_of(f * unit_step, unit_step), unit_step)
            gate_act = jnp.dot(block[...], gate[:, columns], preferred_element_type=jnp.float32)
            up_act = jnp.dot(block[...], up_w[:, columns], preferred_element_type=jnp.float32)
            silu = gate_act / (1.0 + jnp.exp(-gate_act))
            hidden[:, columns] = (silu * up_act).astype(jnp.bfloat16)
            return carry

        lax.fori_loop(0, gate.shape[1] // unit_step, units, 0)
        step = min(FEATURES, width_model)

        def features(f, carry):
            columns = pl.ds(pl.multiple_of(f * step, step), step)
            value = jnp.dot(hidden[...], down[:, columns], preferred_element_type=jnp.float32)
            for t in range(groups):
                piece = value[t * capacity : (t + 1) * capacity]
                partial[t * n + s, :, columns] = piece.astype(jnp.bfloat16)
            return carry

        lax.fori_loop(0, width_model // step, features, 0)
        for chip in range(chips):
            pair_copy(chip, j).start()

    def pair_copy(chip, j):
        return pltpu.make_async_remote_copy(
            src_ref=partial.at[(2 * chip + 1 - core) * n + source_of(j)],
            dst_ref=pair.at[chip * n + j],
            send_sem=pair_send.at[chip * n + j],
            recv_sem=pair_recv.at[chip * n + j],
            device_id={"tp": mate},
            device_id_type=MESH,
        )

    def chip_copy(k, j):
        return pltpu.make_async_remote_copy(
            src_ref=pair.at[(alike[k] // 2) * n + j],
            dst_ref=other.at[k * n + j],
            send_sem=chip_send.at[k * n + j],
            recv_sem=chip_recv.at[k * n + j],
            device_id={"tp": alike[k]},
            device_id_type=MESH,
        )

    def back_copy(j):
        return pltpu.make_async_remote_copy(
            src_ref=done.at[j],
            dst_ref=back.at[me],
            send_sem=back_send.at[j],
            recv_sem=back_recv.at[me],
            device_id={"sp": source_of(j)},
            device_id_type=MESH,
        )

    def sum_pairs(j):
        for chip in range(chips):
            pair_copy(chip, j).wait_recv()
        for k in range(chips - 1):
            chip = alike[k] // 2
            pair[chip * n + j] = (
                partial[alike[k] * n + source_of(j)].astype(jnp.float32)
                + pair[chip * n + j].astype(jnp.float32)
            ).astype(jnp.bfloat16)
        for k in range(chips - 1):
            chip_copy(k, j).start()

    def give_back(j):
        s = source_of(j)
        value = partial[my_t * n + s].astype(jnp.float32) + pair[(my_t // 2) * n + j].astype(
            jnp.float32
        )
        for k in range(chips - 1):
            chip_copy(k, j).wait_recv()
            value = value + other[k * n + j].astype(jnp.float32)
        value = value.astype(jnp.bfloat16)

        @pl.when(s == me)
        def _():
            back[me] = value

        @pl.when(s != me)
        def _():
            done[j] = value
            back_copy(j).start()

    def flow(j, carry):
        pl.when((j >= 4) & (j < n + 4))(lambda: give_back(j - 4))
        pl.when((j >= 3) & (j < n + 3))(lambda: sum_pairs(j - 3))
        pl.when((j >= 2) & (j < n + 2))(lambda: expert(j - 2))
        pl.when(j < n)(lambda: take(j))
        pl.when((j >= 1) & (j < n + 1))(lambda: relay(j - 1))
        return carry

    lax.fori_loop(0, n + 4, flow, 0)

    for h in range(heads):
        sent(0, h, own_ref.at[h])

    def drain(k, carry):
        for h in range(heads):
            sent(2 * k, h, held.at[2 * k * heads + h])
        return carry

    lax.fori_loop(1, level + 1, drain, 0)

    for k in range(1, groups):
        share(k).wait_send()

    def finish(j, carry):
        s = source_of(j)
        pl.when(j >= 1)(lambda: to_expert(j).wait_send())
        for k in range(chips - 1):
            to_chip(k, s, outgoing.at[me]).wait_send()
            to_mate(alike[k], s, outgoing.at[me]).wait_send()
            chip_copy(k, j).wait_send()
        to_mate(my_t, s, outgoing.at[me]).wait_send()
        for chip in range(chips):
            pair_copy(chip, j).wait_send()

        @pl.when(s != me)
        def _():
            back_copy(j).wait_send()
            pltpu.make_async_remote_copy(
                src_ref=done.at[j],
                dst_ref=back.at[s],
                send_sem=back_send.at[j],
                recv_sem=back_recv.at[s],
                device_id={"sp": s},
                device_id_type=MESH,
            ).wait_recv()

        return carry

    lax.fori_loop(0, n, finish, 0)
    extra = [row.astype(jnp.float32) for row in slots]
    extra += [route_weights[k : k + 1, :] for k in range(TOP)]
    extra += [jnp.zeros((8 - len(extra), tokens), jnp.float32)]
    across = jnp.transpose(jnp.concatenate(extra, axis=0))
    slot = lax.broadcasted_iota(jnp.int32, (tokens, n * capacity), 1)
    select = [
        (slot == across[:, k : k + 1].astype(jnp.int32)).astype(jnp.float32).astype(jnp.bfloat16)
        for k in range(TOP)
    ]
    for first in range(0, width_model, wide):
        columns = slice(first, first + wide)
        returned = jnp.concatenate([back[e, :, columns] for e in range(n)], axis=0)
        value = mixed[:, columns].astype(jnp.float32)
        routed = jnp.zeros((tokens, wide), jnp.float32)
        for k in range(TOP):
            picked = jnp.dot(select[k], returned, preferred_element_type=jnp.float32)
            routed = routed + picked * across[:, TOP + k : TOP + k + 1]
        out[:, columns] = (value + routed).astype(out.dtype)


def build_heads(length, heads, queries, keys, values, bias, q_ref, own_ref):
    for h in range(heads):
        columns = slice(h * HEAD_DIM, (h + 1) * HEAD_DIM)
        order = 1 if h % 2 == 0 else -1
        for first in range(0, length, 256):
            rows = slice(first, first + 256)
            query = queries[rows, columns].astype(jnp.float32) * HEAD_DIM ** (-0.5)
            parts = [jnp.zeros_like(query), query][::order]
            q_ref[h, rows, :] = jnp.concatenate(parts, axis=1).astype(jnp.bfloat16)
            parts = [values[rows, columns], keys[rows, columns]][::order]
            parts = [part.astype(jnp.float32) for part in parts]
            own_ref[h, rows, :] = jnp.concatenate(parts, axis=1).astype(jnp.bfloat16)
        line = bias[h : h + 1, :].astype(jnp.float32)
        lines = [line[:, first : first + PAIR] for first in range(0, length, PAIR)]
        lines += [jnp.zeros((BIAS_ROWS - len(lines), PAIR), jnp.float32)]
        own_ref[h, length : length + BIAS_ROWS, :] = jnp.concatenate(lines, axis=0).astype(
            jnp.bfloat16
        )


def slots_of(n, capacity, routes):
    tokens = routes.shape[1]
    expert = lax.broadcasted_iota(jnp.int32, (n, tokens), 0)
    hits = [(expert == routes[k : k + 1, :]).astype(jnp.float32) for k in range(TOP)]
    earlier = lax.broadcasted_iota(jnp.int32, (tokens, tokens), 0) < lax.broadcasted_iota(
        jnp.int32, (tokens, tokens), 1
    )
    before = jnp.dot(
        sum(hits).astype(jnp.bfloat16),
        earlier.astype(jnp.float32).astype(jnp.bfloat16),
        preferred_element_type=jnp.float32,
    )
    start = before + (expert * capacity).astype(jnp.float32)
    return [jnp.sum(hit * start, axis=0, keepdims=True).astype(jnp.int32) for hit in hits]


def take_orders(n):
    orders = [[(me + n - j) % n for j in range(n)] for me in range(n)]
    if n == 8:
        for me, order in [(6, [6, 7, 0, 1, 2, 3, 4, 5]), (7, [7, 6, 1, 0, 3, 2, 5, 4]), (0, [0, 1, 2, 3, 7, 6, 5, 4]), (1, [1, 0, 3, 2, 6, 7, 4, 5]), (4, [4, 5, 3, 2, 1, 0, 7, 6]), (5, [5, 4, 2, 3, 0, 1, 6, 7])]:
            orders[me] = order
    return orders


def greet_all(n, groups, me, my_t):
    barrier = pltpu.get_barrier_semaphore()

    def greet(device):
        pl.semaphore_signal(barrier, inc=1, device_id=device, device_id_type=MESH)

    def greet_sp(r, carry):
        greet({"sp": lax.rem(me + r, n)})
        return carry

    lax.fori_loop(1, n, greet_sp, 0)
    for k in range(1, groups):
        greet({"tp": lax.rem(my_t + k, groups)})


def layer(
    queries, keys, values, bias, routes, route_weights, residual, out_weight, gain, gate, up, down
):
    n, groups = lax.axis_size("sp"), lax.axis_size("tp")
    chips = groups // 2
    length, width = queries.shape
    heads = bias.shape[0]
    tokens, width_model = residual.shape
    capacity = max(2, 5 * tokens * TOP // (4 * n))
    units = gate.shape[1]
    apart = max(1, chips - 1) * n
    vmem = pl.BlockSpec(memory_space=pltpu.VMEM)
    anywhere = pl.BlockSpec(memory_space=pl.ANY)
    kind = queries.dtype
    return pl.pallas_call(
        functools.partial(layer_kernel, n, groups, length, heads),
        out_shape=jax.ShapeDtypeStruct((tokens, width_model), kind),
        in_specs=[vmem] * 6 + [anywhere] * 2 + [vmem] + [anywhere] * 3,
        out_specs=vmem,
        scratch_shapes=[
            pltpu.VMEM((tokens, width_model), kind),
            pltpu.VMEM(out_weight.shape, kind),
            pltpu.VMEM((heads, length, PAIR), kind),
            pltpu.VMEM((heads, length + BIAS_ROWS, PAIR), kind),
            pltpu.VMEM((n * capacity, tokens), kind),
            pltpu.VMEM((n, capacity, width_model), kind),
            pltpu.VMEM((tokens, width_model), kind),
            pltpu.VMEM(((n + 1) * heads, length + BIAS_ROWS, PAIR), kind),
            pltpu.VMEM((heads, length, PAIR), jnp.float32),
            pltpu.VMEM((heads, length, PAIR), jnp.float32),
            pltpu.VMEM((BLOCK, BLOCK), kind),
            pltpu.VMEM((length, width), kind),
            pltpu.VMEM((groups, tokens, width), kind),
            pltpu.VMEM((n, capacity, width_model), kind),
            pltpu.VMEM((groups * n, capacity, width_model), kind),
            pltpu.VMEM((groups * n, capacity, width_model), kind),
            pltpu.VMEM((groups * capacity, width_model), kind),
            pltpu.VMEM((groups * capacity, units), kind),
            pltpu.VMEM((width_model, units), kind),
            pltpu.VMEM((width_model, units), kind),
            pltpu.VMEM((units, width_model), kind),
            pltpu.VMEM((chips * n, capacity, width_model), kind),
            pltpu.VMEM((apart, capacity, width_model), kind),
            pltpu.VMEM((n, capacity, width_model), kind),
            pltpu.SemaphoreType.DMA(((n + 2) * heads,)),
            pltpu.SemaphoreType.DMA(((n + 2) * heads,)),
            pltpu.SemaphoreType.DMA(((n + 2) * heads,)),
            pltpu.SemaphoreType.DMA((groups,)),
            pltpu.SemaphoreType.DMA((groups,)),
            pltpu.SemaphoreType.DMA((5,)),
            pltpu.SemaphoreType.DMA((n,)),
            pltpu.SemaphoreType.DMA((apart,)),
            pltpu.SemaphoreType.DMA((groups * n,)),
            pltpu.SemaphoreType.DMA((groups * n,)),
            pltpu.SemaphoreType.DMA((chips * n,)),
            pltpu.SemaphoreType.DMA((chips * n,)),
            pltpu.SemaphoreType.DMA((apart,)),
            pltpu.SemaphoreType.DMA((apart,)),
            pltpu.SemaphoreType.DMA((n,)),
            pltpu.SemaphoreType.DMA((n,)),
        ],
        compiler_params=pltpu.CompilerParams(
            collective_id=0, has_side_effects=True, vmem_limit_bytes=62 * 1024 * 1024
        ),
        name="layer",
    )(
        queries, keys, values, bias, routes, route_weights, residual, out_weight, gain,
        gate, up, down,
    )


def shards(
    queries,
    keys,
    values,
    key_bias,
    residual,
    out_weight,
    norm_gain,
    routes,
    route_weights,
    gate_weight,
    up_weight,
    down_weight,
):
    return layer(
        queries, keys, values, jnp.transpose(key_bias), jnp.transpose(routes),
        jnp.transpose(route_weights), residual, out_weight, norm_gain[None, :],
        gate_weight[0], up_weight[0], down_weight[0],
    )


def solution(mesh):
    return jax.shard_map(
        shards,
        mesh=mesh,
        in_specs=(
            P("sp", "tp"),
            P("sp", "tp"),
            P("sp", "tp"),
            P("sp", "tp"),
            P(("sp", "tp"), None),
            P(),
            P(),
            P(("sp", "tp"), None),
            P(("sp", "tp"), None),
            P("sp", None, "tp"),
            P("sp", None, "tp"),
            P("sp", "tp", None),
        ),
        out_specs=P(("sp", "tp"), None),
        check_vma=False,
    )
```
